32 devices in a mesh: ep: 4 (over y, x), tp: 8 (over z, core).
Axes of the slice: x: 2, y: 2, z: 4, core: 2. Of those that a mesh axis runs over, the one named last changes fastest.
Arguments:
- resid: bfloat16 [512, 2048], P('ep'), may hold values from -6 to 6
- norm1_gain: float32 [2048], replicated, may hold values from 0.1 to 1.9
- w_query: bfloat16 [2048, 2048], P('ep', 'tp'), may hold values from -0.125 to 0.125
- w_key: bfloat16 [2048, 2048], P('ep', 'tp'), may hold values from -0.125 to 0.125
- w_value: bfloat16 [2048, 2048], P('ep', 'tp'), may hold values from -0.125 to 0.125
- w_outgate: bfloat16 [2048, 2048], P('ep', 'tp'), may hold values from -0.125 to 0.125
- w_igate: bfloat16 [2048, 32], replicated, may hold values from -0.125 to 0.125
- w_fgate: bfloat16 [2048, 32], replicated, may hold values from -0.125 to 0.125
- forget_bias: float32 [32], replicated, may hold values from 0 to 4
- head_gain: float32 [2048], P('tp'), may hold values from 0.1 to 1.9
- w_out: bfloat16 [2048, 2048], P('tp'), may hold values from -0.125 to 0.125
- state_matrix: float32 [512, 32, 64, 64], P('ep', 'tp'), may hold values from -4 to 4
- state_norm: float32 [512, 32, 64], P('ep', 'tp'), may hold values from -8 to 8
- state_max: float32 [512, 32], P('ep', 'tp'), may hold values from -1 to 2
- norm2_gain: float32 [2048], replicated, may hold values from 0.1 to 1.9
- group_router: bfloat16 [2048, 4], replicated, may hold values from -0.125 to 0.125
- expert_router: bfloat16 [2048, 8], replicated, may hold values from -0.125 to 0.125
- expert_ids: int32 [512, 2], P('ep'), may hold values from 0 to 7, all different within a row; in each aligned block of 128 rows (0 to 127, 128 to 255, ...) at most 48 rows name the same one
- exp_gate: bfloat16 [8, 2048, 1024], P('ep', None, 'tp'), may hold values from -0.125 to 0.125
- exp_up: bfloat16 [8, 2048, 1024], P('ep', None, 'tp'), may hold values from -0.125 to 0.125
- exp_down: bfloat16 [8, 1024, 2048], P('ep', 'tp'), may hold values from -0.1875 to 0.1875
Outputs:
- mixed: bfloat16 [512, 2048], P('ep', 'tp')
- new_matrix: float32 [512, 32, 64, 64], P('ep', 'tp')
- new_normer: float32 [512, 32, 64], P('ep', 'tp')
- new_max: float32 [512, 32], P('ep', 'tp')
The draws below stay inside these ranges and needn't reach their ends.
Inputs may be any that keep to these rules, and one draw needn't show every extreme that they name: `expert_ids`: A token's 2 experts differ. Among the 128 tokens of one index of ep (aligned blocks of rows) no expert is named more than 48 times, and in some block one expert is named exactly 48 times.
All inputs are finite; a program needn't handle non-finite values.
Results may differ from the reference program's by a relative error of at most 0.014.
Values may be sent and summed in bfloat16 or wider, within the bound.
A program may use at most 128 MiB of HBM per device.

```python
import math
import jax
import jax.numpy as jnp
import numpy as np
from jax import lax

D = 2048
HEADS = 32
DK = 64
FF = 1024
N_GROUPS = 4
TOPK = 2
SEQ_GRP = 128
TOKENS = 512
EXPERTS = 8
EXP_GROUP = 2
CAP = 48
N_EP = 4


def steps_of(rng, shape, split, low, largest):
    loudness = 1.0
    for axis_at, shards_of in split:
        draws = jax.random.uniform(jax.random.fold_in(jax.random.fold_in(rng, 6), axis_at), (shards_of,), jnp.float32, low / len(split), largest / len(split))
        loudness = loudness * jnp.repeat(jnp.exp(draws), shape[axis_at] // shards_of).reshape((-1,) + (1,) * (len(shape) - 1 - axis_at))
    return loudness


def routed_block(own_key, own, number, rows, amount, top, most, slope):
    order = jax.random.permutation(own_key, amount)
    packed, usual = shares(amount, rows * top, most, slope, True), shares(amount, rows * top, most, slope, False)
    places = jnp.arange(amount)

    def named(tallies, turn):
        used = int((tallies > 0).sum())
        fixed = max(1, used // 4)
        shifted = fixed + (places - fixed + turn * (used - fixed)) % max(1, amount - fixed)
        return jnp.zeros((amount,), jnp.int32).at[order[jnp.where(places < fixed, places, shifted)]].set(jnp.asarray(tallies, jnp.int32))

    tallies = jnp.where(number % 4 == 0, named(packed, number // 4), named(usual, number - number // 4 - 1))
    mixed = jax.random.permutation(jax.random.fold_in(own, 3), amount)
    giver, receiver = mixed[0:amount // 2 * 2:2], mixed[1:amount // 2 * 2:2]
    slack = jnp.minimum(tallies[giver] - 1, most - tallies[receiver]) // 2
    slack = jnp.where((giver == order[0]) | (receiver == order[0]) | (tallies[receiver] == 0), 0, jnp.maximum(slack, 0))
    shifted = jax.random.randint(jax.random.fold_in(own, 4), (amount // 2,), 0, 1 << 20) % (slack + 1)
    tallies = tallies.at[giver].add(-shifted).at[receiver].add(shifted)
    labels = jnp.searchsorted(jnp.cumsum(tallies), jnp.arange(rows * top), side="right").astype(jnp.int32)
    grid = labels.reshape(top, rows).T
    grid = grid[jax.random.permutation(jax.random.fold_in(own, 1), rows)]
    turn = jax.random.randint(jax.random.fold_in(own, 2), (rows, 1), 0, top)
    return jnp.take_along_axis(grid, (jnp.arange(top)[None, :] + turn) % top, axis=1)


def shares(amount, total, bound, slope, full):
    loads = [(1 << 20) // math.isqrt(standing ** slope) + 1 for standing in range(1, amount + 1)]
    largest = bound if full else min(bound, max(-(-total // amount), total * loads[0] // sum(loads)))
    least = 1 if total - largest >= amount - 1 else 0
    holding, surplus = [largest] + [least] * (amount - 1), total - largest - least * (amount - 1)
    while surplus > 0:
        candidates = [i for i in range(1, amount) if holding[i] < largest] or [i for i in range(1, amount) if holding[i] < bound]
        whole, left = sum([loads[i] for i in candidates]), surplus
        for i in candidates:
            more = min(bound - holding[i], max(1, left * loads[i] // whole), surplus)
            holding[i] = holding[i] + more
            surplus = surplus - more
    return np.array(holding)


def normal_values(key, shape, spread, bound, cuts=(), kind=jnp.bfloat16):
    factor_of = steps_of(key, shape, cuts, -0.22, 0.18) if cuts else 1.0
    result = jax.random.normal(key, shape, jnp.float32) * spread * factor_of
    return jnp.minimum(jnp.maximum(result, -bound), bound).astype(kind)


def setup_inputs(seed: int = 0) -> dict:
    keys = jax.random.split(jax.random.key(seed), 22)
    resid = normal_values(keys[0], (TOKENS, D), 1.0, 6.0, ((0, 4),))
    norm1_gain = jnp.clip(1.0 + 0.18 * jax.random.normal(keys[1], (D,), jnp.float32), 0.1, 1.9)
    w_query = normal_values(keys[2], (D, HEADS * DK), D ** -0.5, 0.125, ((0, 4), (1, 8)))
    w_key = normal_values(keys[3], (D, HEADS * DK), D ** -0.5, 0.125, ((0, 4), (1, 8)))
    w_value = normal_values(keys[4], (D, HEADS * DK), D ** -0.5, 0.125, ((0, 4), (1, 8)))
    w_outgate = normal_values(keys[5], (D, HEADS * DK), D ** -0.5, 0.125, ((0, 4), (1, 8)))
    w_igate = normal_values(keys[6], (D, HEADS), D ** -0.5, 0.125)
    w_fgate = normal_values(keys[7], (D, HEADS), D ** -0.5, 0.125)
    forget_bias = jnp.clip(jax.random.uniform(keys[8], (HEADS,), jnp.float32, 0.0, 4.0), 0.0, 4.0)
    head_gain = jnp.clip(1.0 + 0.18 * jax.random.normal(keys[9], (HEADS * DK,), jnp.float32), 0.1, 1.9)
    w_out = normal_values(keys[10], (HEADS * DK, D), (HEADS * DK) ** -0.5, 0.125, ((0, 8),))
    state_matrix = normal_values(keys[11], (TOKENS, HEADS, DK, DK), 0.5, 4.0, ((0, 4), (1, 8)), jnp.float32)
    state_norm = normal_values(keys[12], (TOKENS, HEADS, DK), 2.0, 8.0, ((0, 4), (1, 8)), jnp.float32)
    state_max = jnp.clip(-1.0 + 3.0 * jax.random.uniform(keys[13], (TOKENS, HEADS), jnp.float32) ** steps_of(keys[13], (TOKENS, HEADS), ((0, 4), (1, 8)), -0.2, 0.2), -1.0, 2.0)
    norm2_gain = jnp.clip(1.0 + 0.18 * jax.random.normal(keys[14], (D,), jnp.float32), 0.1, 1.9)
    group_router = normal_values(keys[15], (D, N_GROUPS), D ** -0.5, 0.125)
    expert_router = normal_values(keys[16], (D, EXPERTS), D ** -0.5, 0.125)
    expert_ids_keys = jax.random.split(jax.random.fold_in(keys[17], 1), TOKENS // SEQ_GRP)
    expert_ids_turns = jax.random.permutation(jax.random.fold_in(keys[17], 3), TOKENS // SEQ_GRP)
    expert_ids = jax.vmap(lambda own, number: routed_block(jax.random.fold_in(keys[17], 2), own, number, SEQ_GRP, EXPERTS, TOPK, CAP, 2))(expert_ids_keys, expert_ids_turns).reshape((TOKENS, TOPK))
    exp_gate = normal_values(keys[18], (EXPERTS, D, FF), D ** -0.5, 0.125, ((0, 4), (2, 8)))
    exp_up = normal_values(keys[19], (EXPERTS, D, FF), D ** -0.5, 0.125, ((0, 4), (2, 8)))
    exp_down = normal_values(keys[20], (EXPERTS, FF, D), FF ** -0.5, 0.1875, ((0, 4), (1, 8)))
    return {"resid": resid, "norm1_gain": norm1_gain, "w_query": w_query, "w_key": w_key, "w_value": w_value, "w_outgate": w_outgate, "w_igate": w_igate, "w_fgate": w_fgate, "forget_bias": forget_bias, "head_gain": head_gain, "w_out": w_out, "state_matrix": state_matrix, "state_norm": state_norm, "state_max": state_max, "norm2_gain": norm2_gain, "group_router": group_router, "expert_router": expert_router, "expert_ids": expert_ids, "exp_gate": exp_gate, "exp_up": exp_up, "exp_down": exp_down}


EPSILON = 1e-06

def rms_scale(values, gain):
    widened = values.astype(jnp.float32)
    factor = lax.rsqrt(lax.optimization_barrier(jnp.mean(widened * widened, axis=-1, keepdims=True)) + EPSILON)
    return widened * factor * gain.astype(jnp.float32)

def memory_cell(scaled, key_rows, value_rows, in_gate, log_forget, matrix, normer, running):
    stable = jnp.maximum(log_forget + running, in_gate)
    fresh = jnp.exp(in_gate - stable)
    carried = jnp.exp(log_forget + running - stable)
    readout = jnp.einsum('bhd,bhde->bhe', scaled, matrix, precision=lax.Precision.HIGHEST)
    score = lax.optimization_barrier(jnp.sum(scaled * key_rows, axis=-1)) * fresh
    numer = carried[..., None] * readout + score[..., None] * value_rows
    denom = carried * lax.optimization_barrier(jnp.sum(scaled * normer, axis=-1)) + score
    cell_out = numer / jnp.maximum(jnp.abs(denom), 1.0)[..., None]
    new_matrix = carried[..., None, None] * matrix + fresh[..., None, None] * key_rows[..., :, None] * value_rows[..., None, :]
    new_normer = carried[..., None] * normer + fresh[..., None] * key_rows
    return (cell_out, new_matrix, new_normer, stable)

def reference(resid, norm1_gain, w_query, w_key, w_value, w_outgate, w_igate, w_fgate, forget_bias, head_gain, w_out, state_matrix, state_norm, state_max, norm2_gain, group_router, expert_router, expert_ids, exp_gate, exp_up, exp_down):
    rows = resid.shape[0]
    heads = state_matrix.shape[1]
    size = state_matrix.shape[2]
    normed = rms_scale(resid, norm1_gain).astype(jnp.bfloat16)

    def project(weight):
        product = jnp.dot(normed, weight, preferred_element_type=jnp.float32)
        stored = lax.optimization_barrier(product.astype(jnp.bfloat16))
        return stored.astype(jnp.float32).reshape(rows, heads, size)
    scaled = project(w_query) * size ** (-0.5)
    key_rows = project(w_key)
    value_rows = project(w_value)
    outgate = project(w_outgate)
    in_gate = jnp.dot(normed, w_igate, preferred_element_type=jnp.float32)
    log_forget = jax.nn.log_sigmoid(jnp.dot(normed, w_fgate, preferred_element_type=jnp.float32) + forget_bias)
    cell_out, new_matrix, new_normer, new_max = memory_cell(scaled, key_rows, value_rows, in_gate, log_forget, state_matrix, state_norm, state_max)
    headed = cell_out * lax.rsqrt(lax.optimization_barrier(jnp.mean(cell_out * cell_out, axis=-1, keepdims=True)) + EPSILON)
    headed = headed * head_gain.reshape(heads, size) * jax.nn.sigmoid(outgate)
    head_out = headed.astype(jnp.bfloat16).reshape(rows, heads * size)
    after_mix = (resid.astype(jnp.float32) + jnp.dot(head_out, w_out, preferred_element_type=jnp.float32)).astype(jnp.bfloat16)
    normed2 = rms_scale(after_mix, norm2_gain).astype(jnp.bfloat16)
    group_exp = jnp.exp(jnp.dot(normed2, group_router, preferred_element_type=jnp.float32))
    group_prob = group_exp / lax.optimization_barrier(jnp.sum(group_exp, axis=1, keepdims=True))
    expert_logits = jnp.dot(normed2, expert_router, preferred_element_type=jnp.float32)
    chosen_exp = jnp.exp(jnp.take_along_axis(expert_logits, expert_ids, axis=1))
    share = chosen_exp / lax.optimization_barrier(jnp.sum(chosen_exp, axis=1, keepdims=True))
    group_weight = jnp.take_along_axis(group_prob, expert_ids // EXP_GROUP, axis=1)
    route_weight = group_weight * share
    limit = CAP * N_EP

    def one_expert(total, inputs):
        expert_index, gate_w, up_w, down_w = inputs
        picked = expert_ids == expert_index
        coeff = lax.optimization_barrier(jnp.sum(jnp.where(picked, route_weight, 0.0), axis=1))
        member = jnp.any(picked, axis=1)
        count = jnp.sum(member.astype(jnp.int32))
        places = jnp.nonzero(member, size=limit, fill_value=0)[0].astype(jnp.int32)
        valid = (jnp.arange(limit, dtype=jnp.int32) < count).astype(jnp.float32)
        taken = normed2[places]
        gate_part = jnp.dot(taken, gate_w, preferred_element_type=jnp.float32)
        up_part = jnp.dot(taken, up_w, preferred_element_type=jnp.float32)
        units = (jax.nn.silu(gate_part) * up_part).astype(jnp.bfloat16)
        expert_out = jnp.dot(units, down_w, preferred_element_type=jnp.float32)
        total = total.at[places].add(expert_out * (coeff[places] * valid)[:, None])
        return (total, None)
    start_total = jnp.zeros((rows, resid.shape[1]), jnp.float32)
    moe, _ = lax.scan(one_expert, start_total, (jnp.arange(EXPERTS, dtype=jnp.int32), exp_gate, exp_up, exp_down))
    mixed = (after_mix.astype(jnp.float32) + moe).astype(jnp.bfloat16)
    return (mixed, new_matrix, new_normer, new_max)
```

```python
import functools

import jax
import jax.numpy as jnp
from jax import lax
from jax.experimental import pallas as pl
from jax.experimental.pallas import tpu as pltpu
from jax.sharding import PartitionSpec as P

EPSILON = 1e-06
MESH = pl.DeviceIdType.MESH
VMEM = pl.BlockSpec(memory_space=pltpu.VMEM)
SMEM = pl.BlockSpec(memory_space=pltpu.SMEM)
HBM = pl.BlockSpec(memory_space=pltpu.HBM)
BF16, F32 = jnp.bfloat16, jnp.float32
DMA = pltpu.SemaphoreType.DMA
ROW = (((1,), (1,)), ((), ()))


def remote(src, dst, send_sem, recv_sem, device):
    return pltpu.make_async_remote_copy(
        src_ref=src,
        dst_ref=dst,
        send_sem=send_sem,
        recv_sem=recv_sem,
        device_id=device,
        device_id_type=MESH,
    )


def in_hbm(*arrays):
    return [pltpu.with_memory_space_constraint(a, pltpu.HBM) for a in arrays]


def in_vmem(*arrays):
    return [pltpu.with_memory_space_constraint(a, pltpu.VMEM) for a in arrays]


def greet(devices):
    barrier = pltpu.get_barrier_semaphore()
    for device in devices:
        pl.semaphore_signal(barrier, inc=1, device_id=device, device_id_type=MESH)


def flip(index, mask):
    out, bit = index, 1
    while bit <= mask:
        if mask & bit:
            out = out + bit - 2 * bit * lax.rem(lax.div(index, bit), 2)
        bit *= 2
    return out


def weight_of(mask):
    return bin(mask).count("1")


def dot(a, b):
    return jnp.dot(a, b, preferred_element_type=F32)


def row_dot(a, b):
    return lax.dot_general(a, b, ROW, preferred_element_type=F32)


def columns(index, width):
    return pl.ds(pl.multiple_of(index * width, width), width)


def halving(n, total):
    bits = max(1, n.bit_length() - 1)
    parts = bits if total % (bits * 128) == 0 else 1
    return [[(p + s) % bits for s in range(bits)] for p in range(parts)]


def project_kernel(
    n, resid_h, gain_h, wq, wk, wv, wo, gi_h, gf_h, bias_h, hgain_h, running_h, normer_h,
    state_h, wout_h,
    out, in_gate, log_forget, hgain, running, normer, state, wout,
    resid, gain, gi, gf, bias, weights, blocks, arrived, acc, snd, rcv, gates,
    wsem, fs, fr, ps, pr, rs, rr,
):
    me, t = lax.axis_index("ep"), lax.axis_index("tp")
    c = lax.rem(t, 2)
    partner = {"tp": t + 1 - 2 * c}
    peers = [{"ep": flip(me, r)} for r in range(n)]
    greet(peers[1:] + [partner])
    depth, width = wq.shape
    heads = in_gate.shape[0]
    plan = [(resid_h, resid), (gain_h, gain)]
    for i, w in enumerate((wq, wk, wv, wo)):
        plan.append((w, weights.at[:, i * width : (i + 1) * width]))
    plan += [
        (gi_h, gi), (gf_h, gf), (hgain_h, hgain), (running_h, running), (normer_h, normer),
        (wout_h, wout), (state_h, state), (bias_h, bias),
    ]
    loads = [pltpu.make_async_copy(src, dst, wsem.at[i]) for i, (src, dst) in enumerate(plan)]
    for load in loads:
        load.start()
    loads[0].wait()
    loads[1].wait()
    wide = resid[...].astype(F32)
    factor = lax.rsqrt(jnp.mean(wide * wide, axis=-1, keepdims=True) + EPSILON)
    normed = (wide * factor * gain[...]).astype(BF16)
    for j in range(n):
        blocks[j] = normed[:, j * depth : (j + 1) * depth]
    half = blocks.shape[1] // 2
    mine = pl.ds(pl.multiple_of(c * half, half), half)
    pl.semaphore_wait(pltpu.get_barrier_semaphore(), n)
    order = sorted(range(1, n), key=lambda r: (-weight_of(r), r))
    forward, pass_on = {}, {}
    for r in order:
        forward[r] = remote(
            blocks.at[flip(me, r), mine, :], arrived.at[r, mine, :], fs.at[r], fr.at[r], peers[r]
        )
        forward[r].start()
    for i in range(2, 8):
        loads[i].wait()
    acc[0] = dot(blocks[me], weights[...])
    loads[13].wait()
    for which, g in enumerate((gi, gf)):
        value = row_dot(g[...], normed)
        for j in range(gates.shape[1]):
            gates[which, j] = value[j * heads : (j + 1) * heads]
    in_gate[...] = gates[0, t]
    for j in range(heads):
        log_forget[j : j + 1, :] = jax.nn.log_sigmoid(
            gates[1, t, j : j + 1, :] + bias[t * heads + j]
        )
    for r in order:
        forward[r].wait_recv()
        pass_on[r] = remote(
            arrived.at[r, mine, :], arrived.at[r, mine, :], ps.at[r], pr.at[r], partner
        )
        pass_on[r].start()
    parts = halving(n, 4 * width)
    wide_part = 4 * width // len(parts)
    back = {}

    def summed(p, r, position):
        value = acc[r, :, p * wide_part : (p + 1) * wide_part]
        for s in range(position):
            bit = 1 << parts[p][s]
            back[p, r | bit].wait_recv()
            value = value + rcv[r | bit, p].astype(F32)
        return value

    def position_of(p, r):
        return min(s for s, b in enumerate(parts[p]) if r >> b & 1)

    sends = [(position_of(p, r), -weight_of(r), r, p) for r in range(1, n) for p in range(len(parts))]
    ready = set()
    for position, _, r, p in sorted(sends):
        if r not in ready:
            pass_on[r].wait_recv()
            acc[r] = dot(arrived[r], weights[...])
            ready.add(r)
        snd[r, p] = summed(p, r, position).astype(BF16)
        back[p, r] = remote(
            snd.at[r, p], rcv.at[r, p], rs.at[p, r], rr.at[p, r], peers[1 << parts[p][position]]
        )
        back[p, r].start()
    for i in range(8, 13):
        loads[i].wait()
    for p in range(len(parts)):
        out[:, p * wide_part : (p + 1) * wide_part] = summed(p, 0, len(parts[p])).astype(BF16)
    for r in order:
        forward[r].wait_send()
        pass_on[r].wait_send()
        for p in range(len(parts)):
            back[p, r].wait_send()


def project(
    resid, gain, wq, wk, wv, wo, gi, gf, bias, hgain, running, normer, state, wout
):
    n, nt = lax.axis_size("ep"), lax.axis_size("tp")
    rows, channels = resid.shape
    depth, width = wq.shape
    heads = state.shape[0]
    parts = len(halving(n, 4 * width))
    vmem = pltpu.VMEM
    return pl.pallas_call(
        functools.partial(project_kernel, n),
        out_shape=(
            vmem((rows, 4 * width), BF16),
            vmem(running.shape, F32),
            vmem(running.shape, F32),
            vmem(hgain.shape, F32),
            vmem(running.shape, F32),
            vmem(normer.shape, F32),
            vmem(state.shape, F32),
            vmem(wout.shape, BF16),
        ),
        in_specs=[HBM] * 14,
        out_specs=(VMEM,) * 8,
        scratch_shapes=[
            vmem((rows, channels), BF16),
            vmem((1, channels), F32),
            vmem(gi.shape, BF16),
            vmem(gf.shape, BF16),
            pltpu.SMEM(bias.shape, F32),
            vmem((depth, 4 * width), BF16),
            vmem((n, rows, depth), BF16),
            vmem((n, rows, depth), BF16),
            vmem((n, rows, 4 * width), F32),
            vmem((n, parts, rows, 4 * width // parts), BF16),
            vmem((n, parts, rows, 4 * width // parts), BF16),
            vmem((2, nt, heads, rows), F32),
            DMA((14,)), DMA((n,)), DMA((n,)), DMA((n,)), DMA((n,)),
            DMA((parts, n)), DMA((parts, n)),
        ],
        compiler_params=pltpu.CompilerParams(
            collective_id=0, has_side_effects=True, vmem_limit_bytes=32 * 1024 * 1024
        ),
    )(
        *in_hbm(
            resid, gain, wq, wk, wv, wo, gi, gf, bias, hgain, running, normer, state, wout
        )
    )


def cell_kernel(
    proj, in_gate, log_forget, state, running, normer, hgain,
    new_matrix_h, new_normer_h, new_max_h, head,
    new_matrix, new_normer, new_max, qs, ks, vs, cell, matrix_sem, small_sem,
):
    heads, size = state.shape[:2]
    width = heads * size
    group = 8
    step = min(128, width)

    def store(h, g):
        part = pl.ds(pl.multiple_of(g * group, group), group)
        return pltpu.make_async_copy(
            new_matrix.at[h, part], new_matrix_h.at[h, part], matrix_sem.at[h, g]
        )

    for i, (dst, scale) in enumerate(((qs, size ** (-0.5)), (ks, None), (vs, None))):
        for j in range(0, width, step):
            value = proj[:, i * width + j : i * width + j + step].astype(F32).T
            dst[j : j + step, :] = value if scale is None else value * scale
    for h in range(heads):
        lines = slice(h * size, (h + 1) * size)
        moved = log_forget[h : h + 1, :] + running[h : h + 1, :]
        stable = jnp.maximum(moved, in_gate[h : h + 1, :])
        fresh = jnp.exp(in_gate[h : h + 1, :] - stable)
        carried = jnp.exp(moved - stable)
        new_max[h : h + 1, :] = stable
        q, k = qs[lines, :], ks[lines, :]
        score = jnp.sum(q * k, axis=0, keepdims=True) * fresh
        denom = carried * jnp.sum(q * normer[h], axis=0, keepdims=True) + score
        k = fresh * k
        ks[lines, :] = k
        new_normer[h] = carried * normer[h] + k

        def some(g, readout, h=h, carried=carried):
            start = pl.multiple_of(g * group, group)
            q8 = qs[pl.ds(h * size + start, group), :]
            k8 = ks[pl.ds(h * size + start, group), :]
            v = vs[h * size : (h + 1) * size, :]
            for i in range(group):
                m = state[h, start + i]
                readout = readout + q8[i : i + 1, :] * m
                new_matrix[h, start + i] = carried * m + k8[i : i + 1, :] * v
            store(h, g).start()
            return readout

        readout = lax.fori_loop(0, size // group, some, jnp.zeros(q.shape, F32))
        value = vs[lines, :]
        out = (carried * readout + score * value) / jnp.maximum(jnp.abs(denom), 1.0)
        factor = lax.rsqrt(jnp.mean(out * out, axis=0, keepdims=True) + EPSILON)
        cell[lines, :] = out * factor
    small = [
        pltpu.make_async_copy(src, dst, small_sem.at[i])
        for i, (src, dst) in enumerate(((new_normer, new_normer_h), (new_max, new_max_h)))
    ]
    for copy in small:
        copy.start()
    for j in range(0, width, step):
        gate = jax.nn.sigmoid(proj[:, 3 * width + j : 3 * width + j + step].astype(F32))
        value = cell[j : j + step, :].T * hgain[:, j : j + step] * gate
        head[:, j : j + step] = value.astype(BF16)
    for copy in small:
        copy.wait()
    for h in range(heads):
        lax.fori_loop(0, size // group, lambda g, x, h=h: (store(h, g).wait(), x)[1], 0)


def memory_cell(proj, in_gate, log_forget, state, running, normer, hgain):
    heads, size, _, rows = state.shape
    width = heads * size
    vmem = pltpu.VMEM
    return pl.pallas_call(
        cell_kernel,
        out_shape=(
            pltpu.HBM(state.shape, F32),
            pltpu.HBM(normer.shape, F32),
            pltpu.HBM(running.shape, F32),
            vmem((rows, width), BF16),
        ),
        in_specs=[VMEM] * 7,
        out_specs=(HBM, HBM, HBM, VMEM),
        scratch_shapes=[
            vmem(state.shape, F32),
            vmem(normer.shape, F32),
            vmem(running.shape, F32),
        ]
        + [vmem((width, rows), F32)] * 4
        + [DMA((heads, size // 8)), DMA((2,))],
        compiler_params=pltpu.CompilerParams(vmem_limit_bytes=24 * 1024 * 1024),
    )(*in_vmem(proj, in_gate, log_forget, state, running, normer, hgain))


def expert_kernel(
    n, nt, cap, groups, per_group,
    head, wout, resid_h, gain_h, group_h, router_h, ids_h, wg, wu, wd,
    out,
    own, gain, grouter, router, ids, wgu, wdown, chosen, chosen_r, scatter,
    pair_s, pair_r, red_s, red_r, gathered, disp, arr, stat, stat_r, msg, msg_r,
    hidden, epair_s, epair_r, ret_s, ret_r, z_s, z_r,
    wsem, hs, hr, ps, pr, rs, rr, gs, gr, ds, dr, fs, fr, ss, sr, ms, mr,
    es, er, bs, br, zs, zr,
):
    me, t = lax.axis_index("ep"), lax.axis_index("tp")
    nz = nt // 2
    z, c = lax.div(t, 2), lax.rem(t, 2)
    partner = {"tp": t + 1 - 2 * c}
    peers = [{"ep": flip(me, r)} for r in range(n)]
    z_at = [flip(z, k) for k in range(nz)]
    z_peers = [{"tp": 2 * z_at[k] + c} for k in range(nz)]
    greet([partner] + peers[1:] + z_peers[1:])
    rows, cols = out.shape
    local, ff = wdown.shape[:2]
    experts = n * local
    fused = len(wgu.shape) == 3
    plan = [
        (resid_h.at[:, columns(t, cols)], own),
        (ids_h, ids),
        (gain_h, gain),
        (group_h, grouter),
        (router_h, router),
    ]
    if fused:
        plan += [(wg, wgu.at[:, :, :ff]), (wu, wgu.at[:, :, ff:])]
    else:
        plan += [(wg, wgu.at[0]), (wu, wgu.at[1])]
    plan.append((wd, wdown))
    loads = [pltpu.make_async_copy(src, dst, wsem.at[i]) for i, (src, dst) in enumerate(plan)]
    for load in loads:
        load.start()

    far = sorted(range(1, nz), reverse=True)
    near = list(range(1, nz))
    away = sorted(range(1, n), key=lambda r: (-weight_of(r), r))

    def mixed_block(dest):
        return dot(head[...], wout[:, columns(dest, cols)])

    for k in far + [0]:
        pair_s[k] = mixed_block(2 * z_at[k] + 1 - c).astype(BF16)
    pl.semaphore_wait(pltpu.get_barrier_semaphore(), 1 + (n - 1) + (nz - 1))
    pair = {}
    for k in far + [0]:
        pair[k] = remote(pair_s.at[k], pair_r.at[k], ps.at[k], pr.at[k], partner)
        pair[k].start()

    loads[1].wait()
    expert_id = lax.broadcasted_iota(jnp.int32, (experts, rows), 0)
    picks = [ids[j : j + 1, :] == expert_id for j in range(ids.shape[0])]
    member = functools.reduce(jnp.logical_or, picks)
    member_f = member.astype(F32)
    before = (
        lax.broadcasted_iota(jnp.int32, (rows, rows), 0)
        < lax.broadcasted_iota(jnp.int32, (rows, rows), 1)
    ).astype(BF16)
    slot = dot(member_f.astype(BF16), before)
    slot = jnp.where(member, slot, -1.0)
    slot_id = lax.broadcasted_iota(jnp.int32, (cap, rows), 0).astype(F32)
    hots = []
    for e in range(experts):
        hots.append((slot[e : e + 1, :] == slot_id).astype(F32))
        chosen[e // local, e % local] = hots[e].astype(BF16)

    reduce = {}
    for k in far + [0]:
        value = mixed_block(2 * z_at[k] + c)
        pair[k].wait_recv()
        value = value + pair_r[k].astype(F32)
        if k > 0:
            red_s[k] = value.astype(BF16)
            reduce[k] = remote(red_s.at[k], red_r.at[k], rs.at[k], rr.at[k], z_peers[k])
            reduce[k].start()
        else:
            total = value
    share = {}
    for r in away:
        share[r] = remote(chosen.at[flip(me, r)], chosen_r.at[r], hs.at[r], hr.at[r], peers[r])
        share[r].start()
    for j in range(n):
        block = jnp.concatenate(hots[j * local : (j + 1) * local], axis=0)
        scatter[j] = block.T.astype(BF16)
    loads[0].wait()
    total = total + own[...].astype(F32)
    for i in range(2, 5):
        loads[i].wait()
    for k in near:
        reduce[k].wait_recv()
        total = total + red_r[k].astype(F32)
    gathered[0] = total.astype(BF16)
    gather = {}
    for k in far:
        gather[k] = remote(gathered.at[0], gathered.at[k], gs.at[k], gr.at[k], z_peers[k])
        gather[k].start()

    send, pass_on = {}, {}
    ones = jnp.ones((8, cols), BF16)

    def dispatch(k):
        if k > 0:
            gather[k].wait_recv()
        at = columns(2 * z_at[k] + c, cols)
        raw = gathered[k].astype(F32)
        scaled = (raw * gain[:, at]).astype(BF16)
        taken = dot(chosen[...].reshape(experts * cap, rows), scaled).astype(BF16)
        disp[k] = taken.reshape(n, local, cap, cols)
        for r in away:
            send[k, r] = remote(
                disp.at[k, flip(me, r)], arr.at[c, k, :, r], ds.at[k, r], dr.at[k, r], peers[r]
            )
            send[k, r].start()
        arr[c, k, :, 0] = disp[k, me]
        forward(k, 0)
        square = raw * raw
        high = square.astype(BF16)
        low = (square - high.astype(F32)).astype(BF16)
        parts = (
            row_dot(ones, high) + row_dot(ones, low),
            row_dot(grouter[:, at], scaled),
            row_dot(router[:, at], scaled),
        )
        for base, part in zip((0, 8, 16), parts):
            lines = slice(base, base + part.shape[0])
            if k == 0:
                stat[lines, :] = part
            else:
                stat[lines, :] += part

    def forward(k, r):
        if r > 0:
            send[k, r].wait_recv()
        pass_on[k, r] = remote(
            arr.at[c, k, :, r], arr.at[c, k, :, r], fs.at[k, r], fr.at[k, r], partner
        )
        pass_on[k, r].start()

    def widen(k, side):
        at = columns(2 * z_at[k] + side, cols)
        for e in range(local):
            x = arr[side, k, e].reshape(n * cap, cols)
            if fused:
                parts = [(slice(0, 2 * ff), dot(x, wgu[e, at, :]))]
            else:
                parts = [
                    (slice(i * ff, (i + 1) * ff), dot(x, wgu[i, e, at, :])) for i in range(2)
                ]
            for lanes, part in parts:
                if k == 0 and first[0]:
                    hidden[e, :, lanes] = part
                else:
                    hidden[e, :, lanes] += part

    first = [True]
    dispatch(0)
    for k in near:
        dispatch(k)
        for r in away:
            forward(k - 1, r)
        if k == 1:
            for i in range(5, 8):
                loads[i].wait()
        widen(k - 1, c)
        first[0] = False
        if k > 1:
            for r in range(n):
                pass_on[k - 2, r].wait_recv()
            widen(k - 2, 1 - c)

    swap = remote(stat, stat_r, ss, sr, partner)
    swap.start()
    swap.wait_recv()

    def summed(base, count):
        lines = slice(base, base + count)
        return stat[lines, :] + stat_r[lines, :]

    factor = lax.rsqrt(summed(0, 1) * (1.0 / (cols * nt)) + EPSILON)
    group_exp = jnp.exp(summed(8, groups) * factor)
    group_prob = group_exp / jnp.sum(group_exp, axis=0, keepdims=True)
    logits = summed(16, experts) * factor
    group_id = lax.broadcasted_iota(jnp.int32, (groups, rows), 0)
    chosen_exp = [
        jnp.exp(jnp.sum(jnp.where(pick, logits, 0.0), axis=0, keepdims=True)) for pick in picks
    ]
    denominator = functools.reduce(jnp.add, chosen_exp)
    expert_weight = jnp.zeros((experts, rows), F32)
    for j, pick in enumerate(picks):
        group_hot = lax.div(ids[j : j + 1, :], per_group) == group_id
        group_share = jnp.sum(jnp.where(group_hot, group_prob, 0.0), axis=0, keepdims=True)
        expert_weight += jnp.where(pick, group_share * (chosen_exp[j] / denominator), 0.0)
    for j in range(n):
        msg[j, 0:1, :] = factor
        msg[j, 1 : 1 + local, :] = expert_weight[j * local : (j + 1) * local, :]
    note = {}
    for r in away:
        note[r] = remote(msg.at[flip(me, r)], msg_r.at[r], ms.at[r], mr.at[r], peers[r])
        note[r].start()
    last = nz - 1
    for r in away:
        forward(last, r)
    widen(last, c)
    if nz > 1:
        for r in range(n):
            pass_on[last - 1, r].wait_recv()
        widen(last - 1, 1 - c)
    columns_of = [[], []]
    weights_of = [[], []]
    columns_of = [[] for _ in range(local)]
    weights_of = [[] for _ in range(local)]
    for r in range(n):
        if r > 0:
            share[r].wait_recv()
            note[r].wait_recv()
        for e in range(local):
            hot = (chosen[me, e] if r == 0 else chosen_r[r, e]).astype(F32)
            words = msg[me] if r == 0 else msg_r[r]
            columns_of[e].append(jnp.sum(hot * words[0:1, :], axis=1, keepdims=True))
            weights_of[e].append(jnp.sum(hot * words[1 + e : 2 + e, :], axis=1, keepdims=True))
    for r in range(n):
        pass_on[last, r].wait_recv()
    widen(last, 1 - c)
    units = []
    for e in range(local):
        scale = jnp.concatenate(columns_of[e], axis=0)
        weight = jnp.concatenate(weights_of[e], axis=0)
        gate = hidden[e, :, :ff] * scale
        up = hidden[e, :, ff:] * scale
        units.append((jax.nn.silu(gate) * up * weight).astype(BF16))

    def down(e, dest):
        return dot(units[e], wdown[e, :, columns(dest, cols)])

    epair, ret, gather_z = {}, {}, {}
    for k in far + [0]:
        for e in range(local):
            epair_s[k, e] = down(e, 2 * z_at[k] + 1 - c).astype(BF16).reshape(n, cap, cols)
        epair[k] = remote(epair_s.at[k], epair_r.at[k], es.at[k], er.at[k], partner)
        epair[k].start()
    for k in far + [0]:
        value = [down(e, 2 * z_at[k] + c).reshape(n, cap, cols) for e in range(local)]
        epair[k].wait_recv()
        for e in range(local):
            ret_s[k, e] = (value[e] + epair_r[k, e].astype(F32)).astype(BF16)
        for r in away:
            ret[k, r] = remote(
                ret_s.at[k, :, r], ret_r.at[k, :, r], bs.at[k, r], br.at[k, r], peers[r]
            )
            ret[k, r].start()
    for k in far + [0]:
        total = gathered[0].astype(F32) if k == 0 else None
        for r in [0] + away[::-1]:
            if r > 0:
                ret[k, r].wait_recv()
            back = ret_s[k, :, 0] if r == 0 else ret_r[k, :, r]
            part = dot(scatter[flip(me, r)], back.reshape(local * cap, cols))
            total = part if total is None else total + part
        if k > 0:
            z_s[k] = total.astype(BF16)
            gather_z[k] = remote(z_s.at[k], z_r.at[k], zs.at[k], zr.at[k], z_peers[k])
            gather_z[k].start()
    for k in far:
        gather_z[k].wait_recv()
        total = total + z_r[k].astype(F32)
    out[...] = total.astype(BF16)

    swap.wait_send()
    for k in range(nz):
        pair[k].wait_send()
        epair[k].wait_send()
        for r in range(n):
            pass_on[k, r].wait_send()
            if r > 0:
                send[k, r].wait_send()
                ret[k, r].wait_send()
        if k > 0:
            reduce[k].wait_send()
            gather[k].wait_send()
            gather_z[k].wait_send()
    for r in away:
        share[r].wait_send()
        note[r].wait_send()


def experts_of(head, wout, resid, gain, group_router, expert_router, ids, wg, wu, wd):
    n, nt = lax.axis_size("ep"), lax.axis_size("tp")
    nz = nt // 2
    rows, channels = resid.shape
    cols = channels // nt
    local, _, ff = wg.shape
    experts = n * local
    groups = group_router.shape[0]
    topk = ids.shape[0]
    cap = max(2, 3 * rows * topk // (2 * experts))
    cap = -(-cap // 16) * 16
    lines = 16 + -(-experts // 8) * 8
    words = 1 + local + -(1 + local) % 8
    wide = (local, channels, 2 * ff) if ff % 128 == 0 else (2, local, channels, ff)
    vmem = pltpu.VMEM
    block = (nz, local, n, cap, cols)
    return pl.pallas_call(
        functools.partial(expert_kernel, n, nt, cap, groups, experts // groups),
        out_shape=jax.ShapeDtypeStruct((rows, cols), BF16),
        in_specs=[VMEM] * 2 + [HBM] * 8,
        out_specs=VMEM,
        scratch_shapes=[
            vmem((rows, cols), BF16),
            vmem((1, channels), F32),
            vmem(group_router.shape, BF16),
            vmem(expert_router.shape, BF16),
            vmem(ids.shape, jnp.int32),
            vmem(wide, BF16),
            vmem(wd.shape, BF16),
            vmem((n, local, cap, rows), BF16),
            vmem((n, local, cap, rows), BF16),
            vmem((n, rows, local * cap), BF16),
            vmem((nz, rows, cols), BF16),
            vmem((nz, rows, cols), BF16),
            vmem((nz, rows, cols), BF16),
            vmem((nz, rows, cols), BF16),
            vmem((nz, rows, cols), BF16),
            vmem((nz, n, local, cap, cols), BF16),
            vmem((2,) + block, BF16),
            vmem((lines, rows), F32),
            vmem((lines, rows), F32),
            vmem((n, words, rows), F32),
            vmem((n, words, rows), F32),
            vmem((local, n * cap, 2 * ff), F32),
            vmem(block, BF16),
            vmem(block, BF16),
            vmem(block, BF16),
            vmem(block, BF16),
            vmem((nz, rows, cols), BF16),
            vmem((nz, rows, cols), BF16),
            DMA((8,)), DMA((n,)), DMA((n,)),
            DMA((nz,)), DMA((nz,)), DMA((nz,)), DMA((nz,)), DMA((nz,)), DMA((nz,)),
            DMA((nz, n)), DMA((nz, n)), DMA((nz, n)), DMA((nz, n)),
            DMA, DMA, DMA((n,)), DMA((n,)),
            DMA((nz,)), DMA((nz,)), DMA((nz, n)), DMA((nz, n)), DMA((nz,)), DMA((nz,)),
        ],
        compiler_params=pltpu.CompilerParams(
            collective_id=1, has_side_effects=True, vmem_limit_bytes=40 * 1024 * 1024
        ),
    )(*in_vmem(head, wout), *in_hbm(resid, gain, group_router, expert_router, ids, wg, wu, wd))


def per_device(
    resid,
    norm1_gain,
    w_query,
    w_key,
    w_value,
    w_outgate,
    w_igate,
    w_fgate,
    forget_bias,
    head_gain,
    w_out,
    state_matrix,
    state_norm,
    state_max,
    norm2_gain,
    group_router,
    expert_router,
    expert_ids,
    exp_gate,
    exp_up,
    exp_down,
):
    proj, in_gate, log_forget, hgain, running, normer, state, wout = project(
        resid, norm1_gain.reshape(1, -1), w_query, w_key, w_value, w_outgate,
        w_igate.T, w_fgate.T, forget_bias, head_gain.reshape(1, -1), state_max.T,
        state_norm.transpose(1, 2, 0), state_matrix.transpose(1, 2, 3, 0), w_out,
    )
    new_matrix, new_normer, new_max, head = memory_cell(
        proj, in_gate, log_forget, state, running, normer, hgain
    )
    mixed = experts_of(
        head, wout, resid, norm2_gain.reshape(1, -1), group_router.T, expert_router.T,
        expert_ids.T, exp_gate, exp_up, exp_down,
    )
    return (
        mixed, new_matrix.transpose(3, 0, 1, 2), new_normer.transpose(2, 0, 1), new_max.T
    )


def solution(mesh):
    in_specs = (
        P("ep", None),
        P(),
        P("ep", "tp"),
        P("ep", "tp"),
        P("ep", "tp"),
        P("ep", "tp"),
        P(),
        P(),
        P(),
        P("tp"),
        P("tp", None),
        P("ep", "tp", None, None),
        P("ep", "tp", None),
        P("ep", "tp"),
        P(),
        P(),
        P(),
        P("ep", None),
        P("ep", None, "tp"),
        P("ep", None, "tp"),
        P("ep", "tp", None),
    )
    out_specs = (P("ep", "tp"), P("ep", "tp", None, None), P("ep", "tp", None), P("ep", "tp"))
    return jax.shard_map(
        per_device, mesh=mesh, in_specs=in_specs, out_specs=out_specs, check_vma=False
    )
```

```python
import functools

import jax
import jax.numpy as jnp
from jax import lax
from jax.experimental import pallas as pl
from jax.experimental.pallas import tpu as pltpu
from jax.sharding import PartitionSpec as P

EPSILON = 1e-06
MESH = pl.DeviceIdType.MESH
VMEM = pl.BlockSpec(memory_space=pltpu.VMEM)
SMEM = pl.BlockSpec(memory_space=pltpu.SMEM)
HBM = pl.BlockSpec(memory_space=pltpu.HBM)
BF16, F32 = jnp.bfloat16, jnp.float32
DMA = pltpu.SemaphoreType.DMA
ROW = (((1,), (1,)), ((), ()))


def remote(src, dst, send_sem, recv_sem, device):
    return pltpu.make_async_remote_copy(
        src_ref=src,
        dst_ref=dst,
        send_sem=send_sem,
        recv_sem=recv_sem,
        device_id=device,
        device_id_type=MESH,
    )


def in_hbm(*arrays):
    return [pltpu.with_memory_space_constraint(a, pltpu.HBM) for a in arrays]


def in_vmem(*arrays):
    return [pltpu.with_memory_space_constraint(a, pltpu.VMEM) for a in arrays]


def greet(devices):
    barrier = pltpu.get_barrier_semaphore()
    for device in devices:
        pl.semaphore_signal(barrier, inc=1, device_id=device, device_id_type=MESH)


def flip(index, mask):
    out, bit = index, 1
    while bit <= mask:
        if mask & bit:
            out = out + bit - 2 * bit * lax.rem(lax.div(index, bit), 2)
        bit *= 2
    return out


def weight_of(mask):
    return bin(mask).count("1")


def dot(a, b):
    return jnp.dot(a, b, preferred_element_type=F32)


def row_dot(a, b):
    return lax.dot_general(a, b, ROW, preferred_element_type=F32)


def columns(index, width):
    return pl.ds(pl.multiple_of(index * width, width), width)


def halving(n, total):
    bits = max(1, n.bit_length() - 1)
    parts = bits if total % (bits * 128) == 0 else 1
    return [[(p + s) % bits for s in range(bits)] for p in range(parts)]


def layer_kernel(
    n, nt, cap, groups, per_group,
    resid_h, gain1_h, wq, wk, wv, wo, gi_h, gf_h, bias_h, hgain_h, running_h, normer_h, state_h,
    wout_h, gain2_h, group_h, router_h, ids_h, wg, wu, wd,
    out, new_matrix, new_normer, new_max,
    resid, gain1, gi, gf, bias, hgain, running, normer, state, wout, gain, grouter, router, ids,
    weights, wgu, wdown,
    blocks, arrived, acc, snd, rcv, gates, proj, qs, ks, vs, cell, fades, head,
    own, chosen, chosen_r, scatter,
    pair_s, pair_r, red_s, red_r, gathered, disp, arr, stat, stat_r, msg, msg_r,
    hidden, epair_s, epair_r, ret_s, ret_r, z_s, z_r,
    wsem, as_, ar, qs_, qr, xs, xr,
    hs, hr, ps, pr, rs, rr, gs, gr, ds, dr, fs, fr, ss, sr, ms, mr, es, er, bs, br, zs, zr,
):
    me, t = lax.axis_index("ep"), lax.axis_index("tp")
    nz = nt // 2
    z, c = lax.div(t, 2), lax.rem(t, 2)
    partner = {"tp": t + 1 - 2 * c}
    peers = [{"ep": flip(me, r)} for r in range(n)]
    z_at = [flip(z, k) for k in range(nz)]
    z_peers = [{"tp": 2 * z_at[k] + c} for k in range(nz)]
    greet([partner] + peers[1:] + z_peers[1:])
    rows, cols = out.shape
    local, ff = wdown.shape[:2]
    experts = n * local
    depth, width = wq.shape
    heads, size = state.shape[:2]
    fused = len(wgu.shape) == 3
    batches, lot = snd.shape[0], snd.shape[3]
    lots = [slice(b * lot, (b + 1) * lot) for b in range(batches)]
    far = sorted(range(1, nz), reverse=True)
    near = list(range(1, nz))
    away = sorted(range(1, n), key=lambda r: (-weight_of(r), r))

    plan = {"resid": (resid_h, resid), "gain1": (gain1_h, gain1)}
    for i, w in enumerate((wq, wk, wv, wo)):
        plan[f"w{i}"] = (w, weights.at[:, i * width : (i + 1) * width])
    plan["gi"], plan["gf"], plan["bias"] = (gi_h, gi), (gf_h, gf), (bias_h, bias)
    plan["running"], plan["ids"] = (running_h, running), (ids_h, ids)
    plan["hgain"], plan["normer"] = (hgain_h, hgain), (normer_h, normer)
    plan["state"], plan["wout"] = (state_h, state), (wout_h, wout)
    plan["own"] = (resid_h.at[:, columns(t, cols)], own)
    plan["gain"], plan["group"] = (gain2_h, gain), (group_h, grouter)
    plan["router"] = (router_h, router)
    for i, w in enumerate((wg, wu)):
        plan[f"up{i}"] = (w, wgu.at[:, :, i * ff : (i + 1) * ff] if fused else wgu.at[i])
    plan["down"] = (wd, wdown)
    loads = {
        name: pltpu.make_async_copy(src, dst, wsem.at[i])
        for i, (name, (src, dst)) in enumerate(plan.items())
    }
    for load in loads.values():
        load.start()

    def sent(*kinds):
        for ref, sem in kinds:
            pltpu.make_async_copy(ref, ref, sem).wait()

    def loaded(*names):
        for name in names:
            loads[name].wait()

    loaded("resid", "gain1")
    wide = resid[...].astype(F32)
    factor = lax.rsqrt(jnp.mean(wide * wide, axis=-1, keepdims=True) + EPSILON)
    normed = (wide * factor * gain1[...]).astype(BF16)
    for j in range(n):
        blocks[j] = normed[:, j * depth : (j + 1) * depth]
    half = rows // 2
    mine = pl.ds(pl.multiple_of(c * half, half), half)
    pl.semaphore_wait(pltpu.get_barrier_semaphore(), 1 + (n - 1) + (nz - 1))
    ahead, across = {}, {}
    for r in away:
        ahead[r] = remote(
            blocks.at[flip(me, r), mine, :], arrived.at[r, mine, :], as_, ar.at[r], peers[r]
        )
        ahead[r].start()
    loaded("w0", "w1", "w2", "w3", "gi", "gf", "bias", "running", "ids")
    acc[0] = dot(blocks[me], weights[...])
    for which, g in enumerate((gi, gf)):
        value = row_dot(g[...], normed)
        for j in range(nt):
            gates[which, j] = value[j * heads : (j + 1) * heads]
    for j in range(heads):
        line = slice(j, j + 1)
        in_gate = gates[0, t, line, :]
        forget = jax.nn.log_sigmoid(gates[1, t, line, :] + bias[t * heads + j])
        moved = forget + running[line, :]
        stable = jnp.maximum(moved, in_gate)
        new_max[line, :] = stable
        fades[0, line, :] = jnp.exp(moved - stable)
        fades[1, line, :] = jnp.exp(in_gate - stable)
    proj[...] = jnp.zeros(proj.shape, BF16)
    for r in away:
        ahead[r].wait_recv()
        across[r] = remote(
            arrived.at[r, mine, :], arrived.at[r, mine, :], qs_, qr.at[r], partner
        )
        across[r].start()
    expert_id = lax.broadcasted_iota(jnp.int32, (experts, rows), 0)
    picks = [ids[j : j + 1, :] == expert_id for j in range(ids.shape[0])]
    member = functools.reduce(jnp.logical_or, picks)
    member_f = member.astype(F32)
    before = (
        lax.broadcasted_iota(jnp.int32, (rows, rows), 0)
        < lax.broadcasted_iota(jnp.int32, (rows, rows), 1)
    ).astype(BF16)
    slot = dot(member_f.astype(BF16), before)
    slot = jnp.where(member, slot, -1.0)
    slot_id = lax.broadcasted_iota(jnp.int32, (cap, rows), 0).astype(F32)
    hots = []
    for e in range(experts):
        hots.append((slot[e : e + 1, :] == slot_id).astype(F32))
        chosen[e // local, e % local] = hots[e].astype(BF16)
    for j in range(n):
        block = jnp.concatenate(hots[j * local : (j + 1) * local], axis=0)
        scatter[j] = block.T.astype(BF16)


    parts = halving(n, 4 * width)
    wide_part = 4 * width // len(parts)
    back = {}

    def summed_part(b, p, r, position):
        value = acc[r, lots[b], p * wide_part : (p + 1) * wide_part]
        for s in range(position):
            bit = 1 << parts[p][s]
            back[b, p, r | bit].wait_recv()
            value = value + rcv[b, r | bit, p].astype(F32)
        return value

    steps = {}
    for r in range(1, n):
        for p in range(len(parts)):
            position = min(s for s, bit in enumerate(parts[p]) if r >> bit & 1)
            steps.setdefault((position, -weight_of(r)), []).append((r, p, position))
    order = []
    for i, key in enumerate(sorted(steps)):
        for b in range(batches):
            order.append((max(0, 2 * i - 1) if b == 0 else 2 * i + 2 * b, b, steps[key]))
    ready = {0}
    for _, b, step in sorted(order, key=lambda item: item[:2]):
        for r, p, position in step:
            if r not in ready:
                across[r].wait_recv()
                acc[r] = dot(arrived[r], weights[...])
                ready.add(r)
            snd[b, r, p] = summed_part(b, p, r, position).astype(BF16)
            back[b, p, r] = remote(
                snd.at[b, r, p], rcv.at[b, r, p], xs, xr.at[b, p, r],
                peers[1 << parts[p][position]],
            )
            back[b, p, r].start()

    group = 8
    edge = min(128, heads * size)

    def read(b):
        for p in range(len(parts)):
            value = summed_part(b, p, 0, len(parts[p]))
            proj[lots[b], p * wide_part : (p + 1) * wide_part] = value.astype(BF16)
        for i, dst in enumerate((qs, ks, vs)):
            for j in range(0, width, edge):
                value = proj[:, i * width + j : i * width + j + edge].astype(F32).T
                dst[j : j + edge, :] = value * size ** (-0.5) if i == 0 else value
        for h in range(heads):
            lines = slice(h * size, (h + 1) * size)
            carried, fresh = fades[0, h : h + 1, :], fades[1, h : h + 1, :]
            q = qs[lines, :]
            score = jnp.sum(q * ks[lines, :], axis=0, keepdims=True) * fresh
            denom = carried * jnp.sum(q * normer[h], axis=0, keepdims=True) + score

            def some(g, readout, h=h):
                start = pl.multiple_of(g * group, group)
                q8 = qs[pl.ds(h * size + start, group), :]
                for i in range(group):
                    readout = readout + q8[i : i + 1, :] * state[h, start + i]
                return readout

            readout = lax.fori_loop(0, size // group, some, jnp.zeros(q.shape, F32))
            value = carried * readout + score * vs[lines, :]
            value = value / jnp.maximum(jnp.abs(denom), 1.0)
            mean = jnp.mean(value * value, axis=0, keepdims=True)
            cell[lines, :] = value * lax.rsqrt(mean + EPSILON)
        for j in range(0, width, edge):
            gate = jax.nn.sigmoid(proj[lots[b], 3 * width + j : 3 * width + j + edge].astype(F32))
            value = cell[j : j + edge, :].T[lots[b], :] * hgain[:, j : j + edge] * gate
            head[lots[b], j : j + edge] = value.astype(BF16)

    def renew():
        for h in range(heads):
            lines = slice(h * size, (h + 1) * size)
            carried, fresh = fades[0, h : h + 1, :], fades[1, h : h + 1, :]
            key = fresh * ks[lines, :]
            ks[lines, :] = key
            new_normer[h] = carried * normer[h] + key

            def some(g, x, h=h, carried=carried):
                start = pl.multiple_of(g * group, group)
                k8 = ks[pl.ds(h * size + start, group), :]
                v = vs[h * size : (h + 1) * size, :]
                for i in range(group):
                    new_matrix[h, start + i] = (
                        carried * state[h, start + i] + k8[i : i + 1, :] * v
                    )
                return x

            lax.fori_loop(0, size // group, some, 0)

    pair, reduce, total = {}, {}, {}

    def mixed_block(b, dest):
        return dot(head[lots[b], :], wout[:, columns(dest, cols)])

    def mix(b):
        for k in far + [0]:
            pair_s[b, k] = mixed_block(b, 2 * z_at[k] + 1 - c).astype(BF16)
            pair[b, k] = remote(
                pair_s.at[b, k], pair_r.at[b, k], ps, pr.at[b, k], partner
            )
            pair[b, k].start()
        for k in far + [0]:
            value = mixed_block(b, 2 * z_at[k] + c)
            pair[b, k].wait_recv()
            value = value + pair_r[b, k].astype(F32)
            if k > 0:
                red_s[b, k] = value.astype(BF16)
                reduce[b, k] = remote(
                    red_s.at[b, k], red_r.at[b, k], rs, rr.at[b, k], z_peers[k]
                )
                reduce[b, k].start()
            else:
                total[b] = value + own[lots[b], :].astype(F32)

    loaded("hgain", "normer", "state", "wout", "own")
    for b in range(batches):
        read(b)
        mix(b)
    share = {}
    for r in away:
        share[r] = remote(chosen.at[flip(me, r)], chosen_r.at[r], hs, hr.at[r], peers[r])
        share[r].start()
    renew()
    loaded("gain", "group", "router")
    gather = {}
    for b in range(batches):
        value = total[b]
        for k in near:
            reduce[b, k].wait_recv()
            value = value + red_r[b, k].astype(F32)
        gathered[0, lots[b], :] = value.astype(BF16)
        for k in near:
            gather[b, k] = remote(
                gathered.at[0, lots[b], :], gathered.at[k, lots[b], :],
                gs, gr.at[b, k], z_peers[k],
            )
            gather[b, k].start()

    send, pass_on = {}, {}
    ones = jnp.ones((8, cols), BF16)

    def dispatch(k):
        if k > 0:
            for b in range(batches):
                gather[b, k].wait_recv()
        at = columns(2 * z_at[k] + c, cols)
        raw = gathered[k].astype(F32)
        scaled = (raw * gain[:, at]).astype(BF16)
        taken = dot(chosen[...].reshape(experts * cap, rows), scaled).astype(BF16)
        disp[k] = taken.reshape(n, local, cap, cols)
        for r in away:
            send[k, r] = remote(
                disp.at[k, flip(me, r)], arr.at[c, k, :, r], ds, dr.at[k, r], peers[r]
            )
            send[k, r].start()
        arr[c, k, :, 0] = disp[k, me]
        forward(k, 0)
        square = raw * raw
        high = square.astype(BF16)
        low = (square - high.astype(F32)).astype(BF16)
        parts = (
            row_dot(ones, high) + row_dot(ones, low),
            row_dot(grouter[:, at], scaled),
            row_dot(router[:, at], scaled),
        )
        for base, part in zip((0, 8, 16), parts):
            lines = slice(base, base + part.shape[0])
            if k == 0:
                stat[lines, :] = part
            else:
                stat[lines, :] += part

    def forward(k, r):
        if r > 0:
            send[k, r].wait_recv()
        pass_on[k, r] = remote(
            arr.at[c, k, :, r], arr.at[c, k, :, r], fs, fr.at[k, r], partner
        )
        pass_on[k, r].start()

    def widen(k, side):
        at = columns(2 * z_at[k] + side, cols)
        for e in range(local):
            x = arr[side, k, e].reshape(n * cap, cols)
            if fused:
                parts = [(slice(0, 2 * ff), dot(x, wgu[e, at, :]))]
            else:
                parts = [
                    (slice(i * ff, (i + 1) * ff), dot(x, wgu[i, e, at, :])) for i in range(2)
                ]
            for lanes, part in parts:
                if k == 0 and first[0]:
                    hidden[e, :, lanes] = part
                else:
                    hidden[e, :, lanes] += part

    note, swaps = {}, []

    def announce():
        swap = remote(stat, stat_r, ss, sr, partner)
        swap.start()
        swaps.append(swap)
        swap.wait_recv()

        def summed(base, count):
            lines = slice(base, base + count)
            return stat[lines, :] + stat_r[lines, :]

        factor = lax.rsqrt(summed(0, 1) * (1.0 / (cols * nt)) + EPSILON)
        group_exp = jnp.exp(summed(8, groups) * factor)
        group_prob = group_exp / jnp.sum(group_exp, axis=0, keepdims=True)
        logits = summed(16, experts) * factor
        group_id = lax.broadcasted_iota(jnp.int32, (groups, rows), 0)
        chosen_exp = [
            jnp.exp(jnp.sum(jnp.where(pick, logits, 0.0), axis=0, keepdims=True)) for pick in picks
        ]
        denominator = functools.reduce(jnp.add, chosen_exp)
        expert_weight = jnp.zeros((experts, rows), F32)
        for j, pick in enumerate(picks):
            group_hot = lax.div(ids[j : j + 1, :], per_group) == group_id
            group_share = jnp.sum(jnp.where(group_hot, group_prob, 0.0), axis=0, keepdims=True)
            expert_weight += jnp.where(pick, group_share * (chosen_exp[j] / denominator), 0.0)
        for j in range(n):
            msg[j, 0:1, :] = factor
            msg[j, 1 : 1 + local, :] = expert_weight[j * local : (j + 1) * local, :]
        for r in away:
            note[r] = remote(msg.at[flip(me, r)], msg_r.at[r], ms, mr.at[r], peers[r])
            note[r].start()

    first = [True]
    dispatch(0)
    if nz == 1:
        announce()
    for k in near:
        dispatch(k)
        if k == nz - 1:
            announce()
        for r in away:
            forward(k - 1, r)
        if k == 1:
            loaded("up0", "up1", "down")
        widen(k - 1, c)
        first[0] = False
        if k > 1:
            for r in range(n):
                pass_on[k - 2, r].wait_recv()
            widen(k - 2, 1 - c)

    last = nz - 1
    for r in away:
        forward(last, r)
    widen(last, c)
    if nz > 1:
        for r in range(n):
            pass_on[last - 1, r].wait_recv()
        widen(last - 1, 1 - c)
    columns_of = [[] for _ in range(local)]
    weights_of = [[] for _ in range(local)]
    for r in range(n):
        if r > 0:
            share[r].wait_recv()
            note[r].wait_recv()
        for e in range(local):
            hot = (chosen[me, e] if r == 0 else chosen_r[r, e]).astype(F32)
            words = msg[me] if r == 0 else msg_r[r]
            columns_of[e].append(jnp.sum(hot * words[0:1, :], axis=1, keepdims=True))
            weights_of[e].append(jnp.sum(hot * words[1 + e : 2 + e, :], axis=1, keepdims=True))
    for r in range(n):
        pass_on[last, r].wait_recv()
    widen(last, 1 - c)
    units = []
    for e in range(local):
        scale = jnp.concatenate(columns_of[e], axis=0)
        weight = jnp.concatenate(weights_of[e], axis=0)
        gate = hidden[e, :, :ff] * scale
        up = hidden[e, :, ff:] * scale
        units.append((jax.nn.silu(gate) * up * weight).astype(BF16))

    def down(e, dest):
        return dot(units[e], wdown[e, :, columns(dest, cols)])

    epair, ret, gather_z = {}, {}, {}
    turns = far + [0]

    def offer(k):
        for e in range(local):
            epair_s[k, e] = down(e, 2 * z_at[k] + 1 - c).astype(BF16).reshape(n, cap, cols)
        epair[k] = remote(epair_s.at[k], epair_r.at[k], es, er.at[k], partner)
        epair[k].start()

    offer(turns[0])
    for i, k in enumerate(turns):
        if i + 1 < nz:
            offer(turns[i + 1])
        value = [down(e, 2 * z_at[k] + c).reshape(n, cap, cols) for e in range(local)]
        epair[k].wait_recv()
        for e in range(local):
            ret_s[k, e] = (value[e] + epair_r[k, e].astype(F32)).astype(BF16)
        for r in away:
            ret[k, r] = remote(
                ret_s.at[k, :, r], ret_r.at[k, :, r], bs, br.at[k, r], peers[r]
            )
            ret[k, r].start()
    sent((arrived.at[1:, :half, :], as_), (arrived.at[1:, :half, :], qs_))
    sent((snd.at[:, 1:], xs), (pair_s, ps), (red_s.at[:, 1:], rs), (gathered.at[1:], gs))
    sent((chosen_r.at[1:], hs), (msg_r.at[1:], ms), (disp.at[:, 1:], ds), (arr.at[c], fs))
    sent((stat, ss), (epair_s, es))
    for k in far + [0]:
        total = gathered[0].astype(F32) if k == 0 else None
        for r in [0] + away[::-1]:
            if r > 0:
                ret[k, r].wait_recv()
            back = ret_s[k, :, 0] if r == 0 else ret_r[k, :, r]
            part = dot(scatter[flip(me, r)], back.reshape(local * cap, cols))
            total = part if total is None else total + part
        if k > 0:
            z_s[k] = total.astype(BF16)
            gather_z[k] = remote(z_s.at[k], z_r.at[k], zs, zr.at[k], z_peers[k])
            gather_z[k].start()
    for k in far:
        gather_z[k].wait_recv()
        total = total + z_r[k].astype(F32)
    out[...] = total.astype(BF16)

    sent((ret_s.at[:, :, 1:], bs), (z_s.at[1:], zs))


def layer(
    resid, gain1, wq, wk, wv, wo, gi, gf, bias, hgain, running, normer, state, wout,
    gain2, group_router, expert_router, ids, wg, wu, wd,
):
    n, nt = lax.axis_size("ep"), lax.axis_size("tp")
    nz = nt // 2
    rows, channels = resid.shape
    cols = channels // nt
    depth, width = wq.shape
    heads = state.shape[0]
    local, _, ff = wg.shape
    experts = n * local
    groups = group_router.shape[0]
    topk = ids.shape[0]
    cap = max(2, 3 * rows * topk // (2 * experts))
    cap = -(-cap // 16) * 16
    lines = 16 + -(-experts // 8) * 8
    words = -(-(1 + local) // 8) * 8
    wide = (local, channels, 2 * ff) if ff % 128 == 0 else (2, local, channels, ff)
    parts = len(halving(n, 4 * width))
    batches = 2 if rows % 32 == 0 else 1
    lot = rows // batches
    vmem = pltpu.VMEM
    block = (nz, local, n, cap, cols)
    lot_blocks = (batches, nz, lot, cols)
    returned = (batches, n, parts, lot, 4 * width // parts)
    by_head = (width, rows)
    arrays = (
        resid, gain1, wq, wk, wv, wo, gi, gf, bias, hgain, running, normer, state, wout,
        gain2, group_router, expert_router, ids, wg, wu, wd,
    )
    return pl.pallas_call(
        functools.partial(layer_kernel, n, nt, cap, groups, experts // groups),
        out_shape=(
            vmem((rows, cols), BF16),
            vmem(state.shape, F32),
            vmem(normer.shape, F32),
            vmem(running.shape, F32),
        ),
        in_specs=[HBM] * len(arrays),
        out_specs=(VMEM,) * 4,
        scratch_shapes=[
            vmem((rows, channels), BF16),
            vmem((1, channels), F32),
            vmem(gi.shape, BF16),
            vmem(gf.shape, BF16),
            pltpu.SMEM(bias.shape, F32),
            vmem(hgain.shape, F32),
            vmem(running.shape, F32),
            vmem(normer.shape, F32),
            vmem(state.shape, F32),
            vmem(wout.shape, BF16),
            vmem((1, channels), F32),
            vmem(group_router.shape, BF16),
            vmem(expert_router.shape, BF16),
            vmem(ids.shape, jnp.int32),
            vmem((depth, 4 * width), BF16),
            vmem(wide, BF16),
            vmem(wd.shape, BF16),
            vmem((n, rows, depth), BF16),
            vmem((n, rows, depth), BF16),
            vmem((n, rows, 4 * width), F32),
            vmem(returned, BF16),
            vmem(returned, BF16),
            vmem((2, nt, heads, rows), F32),
            vmem((rows, 4 * width), BF16),
            vmem(by_head, F32),
            vmem(by_head, F32),
            vmem(by_head, F32),
            vmem(by_head, F32),
            vmem((2, heads, rows), F32),
            vmem((rows, width), BF16),
            vmem((rows, cols), BF16),
            vmem((n, local, cap, rows), BF16),
            vmem((n, local, cap, rows), BF16),
            vmem((n, rows, local * cap), BF16),
            vmem(lot_blocks, BF16),
            vmem(lot_blocks, BF16),
            vmem(lot_blocks, BF16),
            vmem(lot_blocks, BF16),
            vmem((nz, rows, cols), BF16),
            vmem((nz, n, local, cap, cols), BF16),
            vmem((2,) + block, BF16),
            vmem((lines, rows), F32),
            vmem((lines, rows), F32),
            vmem((n, words, rows), F32),
            vmem((n, words, rows), F32),
            vmem((local, n * cap, 2 * ff), F32),
            vmem(block, BF16),
            vmem(block, BF16),
            vmem(block, BF16),
            vmem(block, BF16),
            vmem((nz, rows, cols), BF16),
            vmem((nz, rows, cols), BF16),
            DMA((len(arrays) + 1,)),
            DMA, DMA((n,)), DMA, DMA((n,)), DMA, DMA((batches, parts, n)),
            DMA, DMA((n,)), DMA, DMA((batches, nz)), DMA, DMA((batches, nz)),
            DMA, DMA((batches, nz)), DMA, DMA((nz, n)), DMA, DMA((nz, n)),
            DMA, DMA, DMA, DMA((n,)),
            DMA, DMA((nz,)), DMA, DMA((nz, n)), DMA, DMA((nz,)),
        ],
        compiler_params=pltpu.CompilerParams(
            collective_id=0, has_side_effects=True, vmem_limit_bytes=52 * 1024 * 1024
        ),
    )(*in_hbm(*arrays))


def settle_kernel(mixed, matrix, normer, highest, *refs):
    sems = refs[-1]
    pairs = list(zip((mixed, normer, highest), (refs[0], refs[2], refs[3])))
    heads, size = matrix.shape[:2]
    step = size // 4
    for h in range(heads):
        for i in range(0, size, step):
            pairs.append((matrix.at[h, i : i + step], refs[1].at[h, i : i + step]))
    copies = [pltpu.make_async_copy(*pair, sems.at[i]) for i, pair in enumerate(pairs)]
    for copy in copies:
        copy.start()
    for copy in copies:
        copy.wait()


def settle(*arrays):
    return pl.pallas_call(
        settle_kernel,
        out_shape=tuple(pltpu.HBM(a.shape, a.dtype) for a in arrays),
        in_specs=[VMEM] * len(arrays),
        out_specs=(HBM,) * len(arrays),
        scratch_shapes=[DMA((3 + 4 * arrays[1].shape[0],))],
        compiler_params=pltpu.CompilerParams(vmem_limit_bytes=12 * 1024 * 1024),
    )(*in_vmem(*arrays))


def per_device(
    resid,
    norm1_gain,
    w_query,
    w_key,
    w_value,
    w_outgate,
    w_igate,
    w_fgate,
    forget_bias,
    head_gain,
    w_out,
    state_matrix,
    state_norm,
    state_max,
    norm2_gain,
    group_router,
    expert_router,
    expert_ids,
    exp_gate,
    exp_up,
    exp_down,
):
    mixed, new_matrix, new_normer, new_max = settle(
        *layer(
            resid, norm1_gain.reshape(1, -1), w_query, w_key, w_value, w_outgate,
            w_igate.T, w_fgate.T, forget_bias, head_gain.reshape(1, -1), state_max.T,
            state_norm.transpose(1, 2, 0), state_matrix.transpose(1, 2, 3, 0), w_out,
            norm2_gain.reshape(1, -1), group_router.T, expert_router.T, expert_ids.T,
            exp_gate, exp_up, exp_down,
        )
    )
    return (
        mixed, new_matrix.transpose(3, 0, 1, 2), new_normer.transpose(2, 0, 1), new_max.T
    )


def solution(mesh):
    in_specs = (
        P("ep", None),
        P(),
        P("ep", "tp"),
        P("ep", "tp"),
        P("ep", "tp"),
        P("ep", "tp"),
        P(),
        P(),
        P(),
        P("tp"),
        P("tp", None),
        P("ep", "tp", None, None),
        P("ep", "tp", None),
        P("ep", "tp"),
        P(),
        P(),
        P(),
        P("ep", None),
        P("ep", None, "tp"),
        P("ep", None, "tp"),
        P("ep", "tp", None),
    )
    out_specs = (P("ep", "tp"), P("ep", "tp", None, None), P("ep", "tp", None), P("ep", "tp"))
    return jax.shard_map(
        per_device, mesh=mesh, in_specs=in_specs, out_specs=out_specs, check_vma=False
    )
```

```python
import functools

import jax
import jax.numpy as jnp
from jax import lax
from jax.experimental import pallas as pl
from jax.experimental.pallas import tpu as pltpu
from jax.sharding import PartitionSpec as P

EPSILON = 1e-06
MESH = pl.DeviceIdType.MESH
VMEM = pl.BlockSpec(memory_space=pltpu.VMEM)
SMEM = pl.BlockSpec(memory_space=pltpu.SMEM)
HBM = pl.BlockSpec(memory_space=pltpu.HBM)
BF16, F32 = jnp.bfloat16, jnp.float32
DMA = pltpu.SemaphoreType.DMA
ROW = (((1,), (1,)), ((), ()))


def remote(src, dst, send_sem, recv_sem, device):
    return pltpu.make_async_remote_copy(
        src_ref=src,
        dst_ref=dst,
        send_sem=send_sem,
        recv_sem=recv_sem,
        device_id=device,
        device_id_type=MESH,
    )


def in_hbm(*arrays):
    return [pltpu.with_memory_space_constraint(a, pltpu.HBM) for a in arrays]


def in_vmem(*arrays):
    return [pltpu.with_memory_space_constraint(a, pltpu.VMEM) for a in arrays]


def greet(devices):
    barrier = pltpu.get_barrier_semaphore()
    for device in devices:
        pl.semaphore_signal(barrier, inc=1, device_id=device, device_id_type=MESH)


def flip(index, mask):
    out, bit = index, 1
    while bit <= mask:
        if mask & bit:
            out = out + bit - 2 * bit * lax.rem(lax.div(index, bit), 2)
        bit *= 2
    return out


def weight_of(mask):
    return bin(mask).count("1")


def dot(a, b):
    return jnp.dot(a, b, preferred_element_type=F32)


def row_dot(a, b):
    return lax.dot_general(a, b, ROW, preferred_element_type=F32)


def columns(index, width):
    return pl.ds(pl.multiple_of(index * width, width), width)


def halving(n, total):
    bits = max(1, n.bit_length() - 1)
    parts = bits if total % (bits * 128) == 0 else 1
    return [[(p + s) % bits for s in range(bits)] for p in range(parts)]


def layer_kernel(
    n, nt, cap, groups, per_group,
    resid_h, gain1_h, wq, wk, wv, wo, gi_h, gf_h, bias_h, hgain_h, running_h, normer_h, state_h,
    wout_h, gain2_h, group_h, router_h, ids_h, wg, wu, wd,
    out, new_matrix, new_normer, new_max,
    resid, gain1, gi, gf, bias, hgain, running, normer, state, wout, gain, grouter, router, ids,
    weights, wgu, wdown,
    blocks, arrived, acc, snd, rcv, gates, proj, qs, ks, vs, cell, fades, head,
    own, chosen, chosen_r, scatter,
    wout_far, down_give, head_far, units, red_s, red_r, gathered, disp, arr, stat, stat_r, msg, msg_r,
    hidden, ret_s, ret_r, z_s, z_r,
    wsem, as_, ar, qs_, qr, xs, xr,
    hs, hr, ps, pr, ls, lr, rs, rr, gs, gr, ds, dr, fs, fr, ss, sr, ms, mr, es, er, bs, br, zs, zr,
):
    me, t = lax.axis_index("ep"), lax.axis_index("tp")
    nz = nt // 2
    z, c = lax.div(t, 2), lax.rem(t, 2)
    partner = {"tp": t + 1 - 2 * c}
    peers = [{"ep": flip(me, r)} for r in range(n)]
    z_at = [flip(z, k) for k in range(nz)]
    z_peers = [{"tp": 2 * z_at[k] + c} for k in range(nz)]
    greet([partner] + peers[1:] + z_peers[1:])
    rows, cols = out.shape
    local, ff = down_give.shape[1:3]
    experts = n * local
    depth, width = wq.shape
    heads, size = state.shape[:2]
    fused = len(wgu.shape) == 3
    batches, lot = snd.shape[0], snd.shape[3]
    sides, band = disp.shape[0], disp.shape[-1]
    bands = [slice(h * band, (h + 1) * band) for h in range(sides)]
    lots = [slice(b * lot, (b + 1) * lot) for b in range(batches)]
    far = sorted(range(1, nz), reverse=True)
    near = list(range(1, nz))
    away = sorted(range(1, n), key=lambda r: (-weight_of(r), r))

    plan = {"resid": (resid_h, resid), "norm": (gain1_h, gain1)}
    for i, w in enumerate((wq, wk, wv, wo)):
        plan[f"w{i}"] = (w, weights.at[:, i * width : (i + 1) * width])
    together = {"w": weights, "up": wgu, "down": down_give, "give": down_give}
    plan["gi"], plan["gf"], plan["bias"] = (gi_h, gi), (gf_h, gf), (bias_h, bias)
    plan["running"], plan["ids"] = (running_h, running), (ids_h, ids)
    plan["hgain"], plan["normer"] = (hgain_h, hgain), (normer_h, normer)
    plan["state"], plan["wout"] = (state_h, state), (wout_h, wout)
    plan["own"] = (resid_h.at[:, columns(t, cols)], own)
    plan["gain"], plan["group"] = (gain2_h, gain), (group_h, grouter)
    plan["router"] = (router_h, router)
    for i, w in enumerate((wg, wu)):
        plan[f"up{i}"] = (w, wgu.at[:, :, i * ff : (i + 1) * ff] if fused else wgu.at[i])
    for k in range(nz):
        at = columns(2 * z_at[k] + c, cols)
        plan[f"down{k}"] = (wd.at[:, :, at], wdown.at[k, :, :ff, :])
        at = columns(2 * z_at[k] + 1 - c, cols)
        plan[f"give{k}"] = (wd.at[:, :, at], down_give.at[k])
    loads = {}
    for name, (src, dst) in plan.items():
        kind = name.rstrip("0123")
        known = loads.get(kind)
        sem = known[1] if known else wsem.at[len(loads)]
        loads[kind] = (together.get(kind, dst), sem)
        pltpu.make_async_copy(src, dst, sem).start()

    def sent(*kinds):
        for ref, sem in kinds:
            pltpu.make_async_copy(ref, ref, sem).wait()

    def loaded(*names):
        sent(*(loads[name] for name in names))

    loaded("resid", "norm")
    wide = resid[...].astype(F32)
    factor = lax.rsqrt(jnp.mean(wide * wide, axis=-1, keepdims=True) + EPSILON)
    normed = (wide * factor * gain1[...]).astype(BF16)
    for j in range(n):
        blocks[j] = normed[:, j * depth : (j + 1) * depth]
    half = rows // 2
    mine = pl.ds(pl.multiple_of(c * half, half), half)
    pl.semaphore_wait(pltpu.get_barrier_semaphore(), 1 + (n - 1) + (nz - 1))
    ahead, across = {}, {}
    for r in away:
        ahead[r] = remote(
            blocks.at[flip(me, r), mine, :], arrived.at[r, mine, :], as_, ar.at[r - 1], peers[r]
        )
        ahead[r].start()
    loaded("w", "gi", "gf", "bias", "running", "ids")
    acc[0] = dot(blocks[me], weights[...])
    for which, g in enumerate((gi, gf)):
        value = row_dot(g[...], normed)
        for j in range(nt):
            gates[which, j] = value[j * heads : (j + 1) * heads]
    for j in range(heads):
        line = slice(j, j + 1)
        in_gate = gates[0, t, line, :]
        forget = jax.nn.log_sigmoid(gates[1, t, line, :] + bias[t * heads + j])
        moved = forget + running[line, :]
        stable = jnp.maximum(moved, in_gate)
        new_max[line, :] = stable
        fades[0, line, :] = jnp.exp(moved - stable)
        fades[1, line, :] = jnp.exp(in_gate - stable)
    proj[...] = jnp.zeros(proj.shape, BF16)
    for r in away:
        ahead[r].wait_recv()
        across[r] = remote(
            arrived.at[r, mine, :], arrived.at[r, mine, :], qs_, qr.at[r - 1], partner
        )
        across[r].start()
    loaded("wout", "give")
    lend = []
    for k in range(nz):
        at = columns(2 * z_at[k] + 1 - c, cols)
        lend.append(remote(wout.at[:, at], wout_far.at[k], ls.at[0], lr.at[0], partner))
        lend.append(
            remote(down_give.at[k], wdown.at[k, :, ff:, :], ls.at[1], lr.at[1], partner)
        )
    for copy in lend:
        copy.start()
    expert_id = lax.broadcasted_iota(jnp.int32, (experts, rows), 0)
    picks = [ids[j : j + 1, :] == expert_id for j in range(ids.shape[0])]
    member = functools.reduce(jnp.logical_or, picks)
    member_f = member.astype(F32)
    before = (
        lax.broadcasted_iota(jnp.int32, (rows, rows), 0)
        < lax.broadcasted_iota(jnp.int32, (rows, rows), 1)
    ).astype(BF16)
    slot = dot(member_f.astype(BF16), before)
    slot = jnp.where(member, slot, -1.0)
    slot_id = lax.broadcasted_iota(jnp.int32, (cap, rows), 0).astype(F32)
    hots = []
    for e in range(experts):
        hots.append((slot[e : e + 1, :] == slot_id).astype(F32))
        chosen[e // local, e % local] = hots[e].astype(BF16)
    for j in range(n):
        block = jnp.concatenate(hots[j * local : (j + 1) * local], axis=0)
        scatter[j] = block.T.astype(BF16)


    parts = halving(n, 4 * width)
    wide_part = 4 * width // len(parts)
    back = {}

    def summed_part(b, p, r, position):
        value = acc[r, lots[b], p * wide_part : (p + 1) * wide_part]
        for s in range(position):
            bit = 1 << parts[p][s]
            back[b, p, r | bit].wait_recv()
            value = value + rcv[b, r | bit, p].astype(F32)
        return value

    steps = {}
    for r in range(1, n):
        for p in range(len(parts)):
            position = min(s for s, bit in enumerate(parts[p]) if r >> bit & 1)
            steps.setdefault((position, -weight_of(r)), []).append((r, p, position))
    order = []
    for i, key in enumerate(sorted(steps)):
        for b in range(batches):
            order.append((max(0, 2 * i - 1) if b == 0 else 2 * i + 2 * b, b, steps[key]))
    ready = {0}
    for _, b, step in sorted(order, key=lambda item: item[:2]):
        for r, p, position in step:
            if r not in ready:
                across[r].wait_recv()
                acc[r] = dot(arrived[r], weights[...])
                ready.add(r)
            snd[b, r, p] = summed_part(b, p, r, position).astype(BF16)
            back[b, p, r] = remote(
                snd.at[b, r, p], rcv.at[b, r, p], xs, xr.at[b, p, r - 1],
                peers[1 << parts[p][position]],
            )
            back[b, p, r].start()

    group = 8
    edge = min(128, heads * size)

    def read(b):
        for p in range(len(parts)):
            value = summed_part(b, p, 0, len(parts[p]))
            proj[lots[b], p * wide_part : (p + 1) * wide_part] = value.astype(BF16)
        for i, dst in enumerate((qs, ks, vs)):
            for j in range(0, width, edge):
                value = proj[:, i * width + j : i * width + j + edge].astype(F32).T
                dst[j : j + edge, :] = value * size ** (-0.5) if i == 0 else value
        for h in range(heads):
            lines = slice(h * size, (h + 1) * size)
            carried, fresh = fades[0, h : h + 1, :], fades[1, h : h + 1, :]
            q = qs[lines, :]
            score = jnp.sum(q * ks[lines, :], axis=0, keepdims=True) * fresh
            denom = carried * jnp.sum(q * normer[h], axis=0, keepdims=True) + score

            def some(g, readout, h=h):
                start = pl.multiple_of(g * group, group)
                q8 = qs[pl.ds(h * size + start, group), :]
                for i in range(group):
                    readout = readout + q8[i : i + 1, :] * state[h, start + i]
                return readout

            readout = lax.fori_loop(0, size // group, some, jnp.zeros(q.shape, F32))
            value = carried * readout + score * vs[lines, :]
            value = value / jnp.maximum(jnp.abs(denom), 1.0)
            mean = jnp.mean(value * value, axis=0, keepdims=True)
            cell[lines, :] = value * lax.rsqrt(mean + EPSILON)
        for j in range(0, width, edge):
            gate = jax.nn.sigmoid(proj[lots[b], 3 * width + j : 3 * width + j + edge].astype(F32))
            value = cell[j : j + edge, :].T[lots[b], :] * hgain[:, j : j + edge] * gate
            head[lots[b], j : j + edge] = value.astype(BF16)

    def renew():
        for h in range(heads):
            lines = slice(h * size, (h + 1) * size)
            carried, fresh = fades[0, h : h + 1, :], fades[1, h : h + 1, :]
            key = fresh * ks[lines, :]
            ks[lines, :] = key
            new_normer[h] = carried * normer[h] + key

            def some(g, x, h=h, carried=carried):
                start = pl.multiple_of(g * group, group)
                k8 = ks[pl.ds(h * size + start, group), :]
                v = vs[h * size : (h + 1) * size, :]
                for i in range(group):
                    new_matrix[h, start + i] = (
                        carried * state[h, start + i] + k8[i : i + 1, :] * v
                    )
                return x

            lax.fori_loop(0, size // group, some, 0)

    pair, reduce, total = {}, {}, {}

    def mix(b):
        pair[b] = remote(
            head.at[lots[b], :], head_far.at[lots[b], :], ps, pr.at[b], partner
        )
        pair[b].start()
        values = {}
        for k in far + [0]:
            at = columns(2 * z_at[k] + c, cols)
            values[k] = dot(head[lots[b], :], wout[:, at])
        pair[b].wait_recv()
        for k in far + [0]:
            value = values[k] + dot(head_far[lots[b], :], wout_far[k])
            if k > 0:
                for h in range(sides):
                    red_s[b, k, h] = value[:, bands[h]].astype(BF16)
            else:
                total[b] = value + own[lots[b], :].astype(F32)
        for h in range(sides):
            for k in far:
                reduce[b, k, h] = remote(
                    red_s.at[b, k, h], red_r.at[b, k, h], rs, rr.at[b, k - 1, h], z_peers[k]
                )
                reduce[b, k, h].start()

    loaded("hgain", "normer", "state", "own")
    sent((wout_far, lr.at[0]))
    for b in range(batches):
        read(b)
        mix(b)
    share = {}
    for r in away:
        share[r] = remote(chosen.at[flip(me, r)], chosen_r.at[r], hs, hr.at[r - 1], peers[r])
        share[r].start()
    renew()
    loaded("gain", "group", "router")
    gather = {}

    def collect(h):
        for b in range(batches):
            value = total[b][:, bands[h]]
            for k in near:
                reduce[b, k, h].wait_recv()
                value = value + red_r[b, k, h].astype(F32)
            gathered[h, 0, lots[b], :] = value.astype(BF16)
        for k in near:
            gather[h, k] = remote(
                gathered.at[h, 0], gathered.at[h, k], gs, gr.at[h, k - 1], z_peers[k]
            )
            gather[h, k].start()

    send, pass_on = {}, {}
    ones = jnp.ones((8, band), BF16)

    def lanes_of(h, k, side):
        start = (2 * z_at[k] + side) * cols + h * band
        return pl.ds(pl.multiple_of(start, band), band)

    def dispatch(h, k):
        if k > 0:
            gather[h, k].wait_recv()
        at = lanes_of(h, k, c)
        raw = gathered[h, k].astype(F32)
        scaled = (raw * gain[:, at]).astype(BF16)
        taken = dot(chosen[...].reshape(experts * cap, rows), scaled).astype(BF16)
        disp[h, k] = taken.reshape(n, local, cap, band)
        for r in away:
            send[h, k, r] = remote(
                disp.at[h, k, flip(me, r)], arr.at[c, h, k, :, r], ds, dr.at[h, k], peers[r]
            )
            send[h, k, r].start()
        arr[c, h, k, :, 0] = disp[h, k, me]
        square = raw * raw
        high = square.astype(BF16)
        low = (square - high.astype(F32)).astype(BF16)
        parts = (
            row_dot(ones, high) + row_dot(ones, low),
            row_dot(grouter[:, at], scaled),
            row_dot(router[:, at], scaled),
        )
        for base, part in zip((0, 8, 16), parts):
            lines = slice(base, base + part.shape[0])
            if k + h == 0:
                stat[lines, :] = part
            else:
                stat[lines, :] += part

    def forward(h, k):
        ref = arr.at[c, h, k, :, 1:]
        sent((ref, dr.at[h, k]))
        ref = arr.at[c, h, k]
        pass_on[h, k] = remote(ref, ref, fs, fr.at[h, k], partner)
        pass_on[h, k].start()
        widen(h, k, c)

    def settle_pass(h, k):
        pass_on[h, k].wait_recv()
        widen(h, k, 1 - c)

    def widen(h, k, side):
        at = lanes_of(h, k, side)
        for e in range(local):
            x = arr[side, h, k, e].reshape(n * cap, band)
            if fused:
                parts = [(slice(0, 2 * ff), dot(x, wgu[e, at, :]))]
            else:
                parts = [
                    (slice(i * ff, (i + 1) * ff), dot(x, wgu[i, e, at, :])) for i in range(2)
                ]
            for lanes, part in parts:
                if first[0]:
                    hidden[e, :, lanes] = part
                else:
                    hidden[e, :, lanes] += part
        first[0] = False

    note, swaps = {}, []

    def announce():
        swap = remote(stat, stat_r, ss, sr, partner)
        swap.start()
        swaps.append(swap)
        swap.wait_recv()

        def summed(base, count):
            lines = slice(base, base + count)
            return stat[lines, :] + stat_r[lines, :]

        factor = lax.rsqrt(summed(0, 1) * (1.0 / (cols * nt)) + EPSILON)
        group_exp = jnp.exp(summed(8, groups) * factor)
        group_prob = group_exp / jnp.sum(group_exp, axis=0, keepdims=True)
        logits = summed(16, experts) * factor
        group_id = lax.broadcasted_iota(jnp.int32, (groups, rows), 0)
        chosen_exp = [
            jnp.exp(jnp.sum(jnp.where(pick, logits, 0.0), axis=0, keepdims=True)) for pick in picks
        ]
        denominator = functools.reduce(jnp.add, chosen_exp)
        expert_weight = jnp.zeros((experts, rows), F32)
        for j, pick in enumerate(picks):
            group_hot = lax.div(ids[j : j + 1, :], per_group) == group_id
            group_share = jnp.sum(jnp.where(group_hot, group_prob, 0.0), axis=0, keepdims=True)
            expert_weight += jnp.where(pick, group_share * (chosen_exp[j] / denominator), 0.0)
        for j in range(n):
            msg[j, 0:1, :] = factor
            msg[j, 1 : 1 + local, :] = expert_weight[j * local : (j + 1) * local, :]
        for r in away:
            note[r] = remote(msg.at[flip(me, r)], msg_r.at[r], ms, mr.at[r - 1], peers[r])
            note[r].start()

    first = [True]
    items = [(h, 0) for h in range(sides)]
    items += [(h, k) for h in range(sides) for k in near]
    for i, (h, k) in enumerate(items):
        if k == 0:
            collect(h)
        dispatch(h, k)
    announce()
    loaded("up")
    for i in range(len(items)):
        forward(*items[i])
        if i > 0:
            settle_pass(*items[i - 1])
    columns_of = [[] for _ in range(local)]
    weights_of = [[] for _ in range(local)]
    for r in range(n):
        if r > 0:
            share[r].wait_recv()
            note[r].wait_recv()
        for e in range(local):
            hot = (chosen[me, e] if r == 0 else chosen_r[r, e]).astype(F32)
            words = msg[me] if r == 0 else msg_r[r]
            columns_of[e].append(jnp.sum(hot * words[0:1, :], axis=1, keepdims=True))
            weights_of[e].append(jnp.sum(hot * words[1 + e : 2 + e, :], axis=1, keepdims=True))
    settle_pass(*items[-1])
    share_units = []
    for e in range(local):
        scale = jnp.concatenate(columns_of[e], axis=0)
        weight = jnp.concatenate(weights_of[e], axis=0)
        gate = hidden[e, :, :ff] * scale
        up = hidden[e, :, ff:] * scale
        units[0, e] = (jax.nn.silu(gate) * up * weight).astype(BF16)
        copy = remote(units.at[0, e], units.at[1, e], es, er.at[e], partner)
        copy.start()
        share_units.append(copy)

    loaded("down")
    sent((down_give, lr.at[1]))
    for copy in share_units:
        copy.wait_recv()
    ret, gather_z = {}, {}
    if ff % 128 == 0:
        both = [jnp.concatenate([units[0, e], units[1, e]], axis=1) for e in range(local)]
    for k in far + [0]:
        for e in range(local):
            if ff % 128 == 0:
                value = dot(both[e], wdown[k, e])
            else:
                value = dot(units[0, e], wdown[k, e, :ff, :]) + dot(
                    units[1, e], wdown[k, e, ff:, :]
                )
            value = value.astype(BF16).reshape(n, cap, cols)
            for h in range(sides):
                ret_s[k, h, e] = value[:, :, bands[h]]
        for h in range(sides):
            for r in away:
                ret[k, h, r] = remote(
                    ret_s.at[k, h, :, r], ret_r.at[k, h, :, r], bs, br.at[k, h], peers[r]
                )
                ret[k, h, r].start()
    sent((arrived.at[1:, :half, :], as_), (arrived.at[1:, :half, :], qs_))
    sent((snd.at[:, 1:], xs), (head, ps), (red_s.at[:, 1:], rs), (gathered.at[:, 1:], gs))
    sent((chosen_r.at[1:], hs), (msg_r.at[1:], ms), (disp.at[:, :, 1:], ds), (arr.at[c], fs))
    sent((stat, ss), (units.at[0], es), (wout_far, ls.at[0]), (down_give, ls.at[1]))
    for k in far + [0]:
        for h in range(sides):
            total = gathered[h, 0].astype(F32) if k == 0 else None
            sent((ret_r.at[k, h, :, 1:], br.at[k, h]))
            for r in range(n):
                answer = ret_s[k, h, :, 0] if r == 0 else ret_r[k, h, :, r]
                part = dot(scatter[flip(me, r)], answer.reshape(local * cap, band))
                total = part if total is None else total + part
            if k > 0:
                z_s[k, h] = total.astype(BF16)
                gather_z[k, h] = remote(
                    z_s.at[k, h], z_r.at[k, h], zs, zr.at[k - 1, h], z_peers[k]
                )
                gather_z[k, h].start()
            else:
                for k_from in far:
                    gather_z[k_from, h].wait_recv()
                    total = total + z_r[k_from, h].astype(F32)
                out[:, bands[h]] = total.astype(BF16)
    sent((ret_s.at[:, :, :, 1:], bs), (z_s.at[1:], zs))


def layer(
    resid, gain1, wq, wk, wv, wo, gi, gf, bias, hgain, running, normer, state, wout,
    gain2, group_router, expert_router, ids, wg, wu, wd,
):
    n, nt = lax.axis_size("ep"), lax.axis_size("tp")
    nz = nt // 2
    rows, channels = resid.shape
    cols = channels // nt
    depth, width = wq.shape
    heads = state.shape[0]
    local, _, ff = wg.shape
    experts = n * local
    groups = group_router.shape[0]
    topk = ids.shape[0]
    cap = max(2, 3 * rows * topk // (2 * experts))
    cap = -(-cap // 16) * 16
    lines = 16 + -(-experts // 8) * 8
    words = -(-(1 + local) // 8) * 8
    wide = (local, channels, 2 * ff) if ff % 128 == 0 else (2, local, channels, ff)
    parts = len(halving(n, 4 * width))
    batches = 2 if rows % 32 == 0 else 1
    lot = rows // batches
    vmem = pltpu.VMEM
    sides = 2 if cols % 256 == 0 else 1
    band = cols // sides
    reduced = (batches, nz, sides, lot, band)
    returned = (batches, n, parts, lot, 4 * width // parts)
    by_head = (width, rows)
    arrays = (
        resid, gain1, wq, wk, wv, wo, gi, gf, bias, hgain, running, normer, state, wout,
        gain2, group_router, expert_router, ids, wg, wu, wd,
    )
    return pl.pallas_call(
        functools.partial(layer_kernel, n, nt, cap, groups, experts // groups),
        out_shape=(
            vmem((rows, cols), BF16),
            vmem(state.shape, F32),
            vmem(normer.shape, F32),
            vmem(running.shape, F32),
        ),
        in_specs=[HBM] * len(arrays),
        out_specs=(VMEM,) * 4,
        scratch_shapes=[
            vmem((rows, channels), BF16),
            vmem((1, channels), F32),
            vmem(gi.shape, BF16),
            vmem(gf.shape, BF16),
            pltpu.SMEM(bias.shape, F32),
            vmem(hgain.shape, F32),
            vmem(running.shape, F32),
            vmem(normer.shape, F32),
            vmem(state.shape, F32),
            vmem(wout.shape, BF16),
            vmem((1, channels), F32),
            vmem(group_router.shape, BF16),
            vmem(expert_router.shape, BF16),
            vmem(ids.shape, jnp.int32),
            vmem((depth, 4 * width), BF16),
            vmem(wide, BF16),
            vmem((nz, local, 2 * ff, cols), BF16),
            vmem((n, rows, depth), BF16),
            vmem((n, rows, depth), BF16),
            vmem((n, rows, 4 * width), F32),
            vmem(returned, BF16),
            vmem(returned, BF16),
            vmem((2, nt, heads, rows), F32),
            vmem((rows, 4 * width), BF16),
            vmem(by_head, F32),
            vmem(by_head, F32),
            vmem(by_head, F32),
            vmem(by_head, F32),
            vmem((2, heads, rows), F32),
            vmem((rows, width), BF16),
            vmem((rows, cols), BF16),
            vmem((n, local, cap, rows), BF16),
            vmem((n, local, cap, rows), BF16),
            vmem((n, rows, local * cap), BF16),
            vmem((nz, width, cols), BF16),
            vmem((nz, local, ff, cols), BF16),
            vmem((rows, width), BF16),
            vmem((2, local, n * cap, ff), BF16),
            vmem(reduced, BF16),
            vmem(reduced, BF16),
            vmem((sides, nz, rows, band), BF16),
            vmem((sides, nz, n, local, cap, band), BF16),
            vmem((2, sides, nz, local, n, cap, band), BF16),
            vmem((lines, rows), F32),
            vmem((lines, rows), F32),
            vmem((n, words, rows), F32),
            vmem((n, words, rows), F32),
            vmem((local, n * cap, 2 * ff), F32),
            vmem((nz, sides, local, n, cap, band), BF16),
            vmem((nz, sides, local, n, cap, band), BF16),
            vmem((nz, sides, rows, band), BF16),
            vmem((nz, sides, rows, band), BF16),
            DMA((len(arrays),)),
            DMA, DMA((n - 1,)), DMA, DMA((n - 1,)), DMA, DMA((batches, parts, n - 1)),
            DMA, DMA((n - 1,)), DMA, DMA((batches,)), DMA((2,)), DMA((2,)),
            DMA, DMA((batches, nz - 1, sides)),
            DMA, DMA((sides, nz - 1)), DMA, DMA((sides, nz)), DMA, DMA((sides, nz)),
            DMA, DMA, DMA, DMA((n - 1,)),
            DMA, DMA((local,)), DMA, DMA((nz, sides)), DMA, DMA((nz - 1, sides)),
        ],
        compiler_params=pltpu.CompilerParams(
            collective_id=0, has_side_effects=True, vmem_limit_bytes=52 * 1024 * 1024
        ),
    )(*in_hbm(*arrays))


def settle_kernel(mixed, matrix, normer, highest, *refs):
    sems = refs[-1]
    pairs = list(zip((mixed, normer, highest), (refs[0], refs[2], refs[3])))
    heads, size = matrix.shape[:2]
    step = size // 4
    for h in range(heads):
        for i in range(0, size, step):
            pairs.append((matrix.at[h, i : i + step], refs[1].at[h, i : i + step]))
    copies = [pltpu.make_async_copy(*pair, sems.at[i]) for i, pair in enumerate(pairs)]
    for copy in copies:
        copy.start()
    for copy in copies:
        copy.wait()


def settle(*arrays):
    return pl.pallas_call(
        settle_kernel,
        out_shape=tuple(pltpu.HBM(a.shape, a.dtype) for a in arrays),
        in_specs=[VMEM] * len(arrays),
        out_specs=(HBM,) * len(arrays),
        scratch_shapes=[DMA((3 + 4 * arrays[1].shape[0],))],
        compiler_params=pltpu.CompilerParams(vmem_limit_bytes=12 * 1024 * 1024),
    )(*in_vmem(*arrays))


def per_device(
    resid,
    norm1_gain,
    w_query,
    w_key,
    w_value,
    w_outgate,
    w_igate,
    w_fgate,
    forget_bias,
    head_gain,
    w_out,
    state_matrix,
    state_norm,
    state_max,
    norm2_gain,
    group_router,
    expert_router,
    expert_ids,
    exp_gate,
    exp_up,
    exp_down,
):
    mixed, new_matrix, new_normer, new_max = settle(
        *layer(
            resid, norm1_gain.reshape(1, -1), w_query, w_key, w_value, w_outgate,
            w_igate.T, w_fgate.T, forget_bias, head_gain.reshape(1, -1), state_max.T,
            state_norm.transpose(1, 2, 0), state_matrix.transpose(1, 2, 3, 0), w_out,
            norm2_gain.reshape(1, -1), group_router.T, expert_router.T, expert_ids.T,
            exp_gate, exp_up, exp_down,
        )
    )
    return (
        mixed, new_matrix.transpose(3, 0, 1, 2), new_normer.transpose(2, 0, 1), new_max.T
    )


def solution(mesh):
    in_specs = (
        P("ep", None),
        P(),
        P("ep", "tp"),
        P("ep", "tp"),
        P("ep", "tp"),
        P("ep", "tp"),
        P(),
        P(),
        P(),
        P("tp"),
        P("tp", None),
        P("ep", "tp", None, None),
        P("ep", "tp", None),
        P("ep", "tp"),
        P(),
        P(),
        P(),
        P("ep", None),
        P("ep", None, "tp"),
        P("ep", None, "tp"),
        P("ep", "tp", None),
    )
    out_specs = (P("ep", "tp"), P("ep", "tp", None, None), P("ep", "tp", None), P("ep", "tp"))
    return jax.shard_map(
        per_device, mesh=mesh, in_specs=in_specs, out_specs=out_specs, check_vma=False
    )
```

```python
import functools

import jax
import jax.numpy as jnp
from jax import lax
from jax.experimental import pallas as pl
from jax.experimental.pallas import tpu as pltpu
from jax.sharding import PartitionSpec as P

EPSILON = 1e-06
MESH = pl.DeviceIdType.MESH
VMEM = pl.BlockSpec(memory_space=pltpu.VMEM)
SMEM = pl.BlockSpec(memory_space=pltpu.SMEM)
HBM = pl.BlockSpec(memory_space=pltpu.HBM)
BF16, F32 = jnp.bfloat16, jnp.float32
DMA = pltpu.SemaphoreType.DMA
ROW = (((1,), (1,)), ((), ()))


def remote(src, dst, send_sem, recv_sem, device):
    return pltpu.make_async_remote_copy(
        src_ref=src,
        dst_ref=dst,
        send_sem=send_sem,
        recv_sem=recv_sem,
        device_id=device,
        device_id_type=MESH,
    )


def in_hbm(*arrays):
    return [pltpu.with_memory_space_constraint(a, pltpu.HBM) for a in arrays]


def in_vmem(*arrays):
    return [pltpu.with_memory_space_constraint(a, pltpu.VMEM) for a in arrays]


def greet(devices):
    barrier = pltpu.get_barrier_semaphore()
    for device in devices:
        pl.semaphore_signal(barrier, inc=1, device_id=device, device_id_type=MESH)


def flip(index, mask):
    out, bit = index, 1
    while bit <= mask:
        if mask & bit:
            out = out + bit - 2 * bit * lax.rem(lax.div(index, bit), 2)
        bit *= 2
    return out


def weight_of(mask):
    return bin(mask).count("1")


def dot(a, b):
    return jnp.dot(a, b, preferred_element_type=F32)


def row_dot(a, b):
    return lax.dot_general(a, b, ROW, preferred_element_type=F32)


def columns(index, width):
    return pl.ds(pl.multiple_of(index * width, width), width)


def halving(n, total):
    bits = max(1, n.bit_length() - 1)
    parts = bits if total % (bits * 128) == 0 else 1
    return [[(p + s) % bits for s in range(bits)] for p in range(parts)]


def layer_kernel(
    n, nt, cap, groups, per_group,
    resid_h, gain1_h, wq, wk, wv, wo, gi_h, gf_h, bias_h, hgain_h, running_h, normer_h, state_h,
    wout_h, gain2_h, group_h, router_h, ids_h, wg, wu, wd,
    out, new_matrix, new_normer, new_max,
    resid, gain1, gi, gf, bias, hgain, running, normer, state, wout, gain, grouter, router, ids,
    weights, wgu, wdown,
    blocks, arrived, acc, snd, rcv, gates, proj, qs, ks, vs, cell, fades, head,
    own, chosen, chosen_r, scatter,
    wout_far, down_give, head_far, units, red_s, red_r, gathered, disp, arr, stat, stat_r, msg, msg_r,
    hidden, ret_s, ret_r, z_s, z_r,
    wsem, as_, ar, qs_, qr, xs, xr,
    hs, hr, ps, pr, ls, lr, rs, rr, gs, gr, ds, dr, fs, fr, ss, sr, ms, mr, es, er, bs, br, zs, zr,
):
    me, t = lax.axis_index("ep"), lax.axis_index("tp")
    nz = nt // 2
    z, c = lax.div(t, 2), lax.rem(t, 2)
    partner = {"tp": t + 1 - 2 * c}
    peers = [{"ep": flip(me, r)} for r in range(n)]
    z_at = [flip(z, k) for k in range(nz)]
    z_peers = [{"tp": 2 * z_at[k] + c} for k in range(nz)]
    greet([partner] + peers[1:] + z_peers[1:])
    rows, cols = out.shape
    local, ff = down_give.shape[1:3]
    experts = n * local
    depth, width = wq.shape
    heads, size = state.shape[:2]
    fused = len(wgu.shape) == 3
    batches, lot = snd.shape[0], snd.shape[3]
    sides, band = disp.shape[0], disp.shape[-1]
    bands = [slice(h * band, (h + 1) * band) for h in range(sides)]
    lots = [slice(b * lot, (b + 1) * lot) for b in range(batches)]
    far = sorted(range(1, nz), reverse=True)
    near = list(range(1, nz))
    away = sorted(range(1, n), key=lambda r: (-weight_of(r), r))

    plan = {"resid": (resid_h, resid), "norm": (gain1_h, gain1)}
    for i, w in enumerate((wq, wk, wv, wo)):
        plan[f"w{i}"] = (w, weights.at[:, i * width : (i + 1) * width])
    together = {"w": weights, "up": wgu, "down": down_give, "give": down_give}
    plan["gi"], plan["gf"], plan["bias"] = (gi_h, gi), (gf_h, gf), (bias_h, bias)
    plan["running"], plan["ids"] = (running_h, running), (ids_h, ids)
    plan["hgain"], plan["normer"] = (hgain_h, hgain), (normer_h, normer)
    plan["state"], plan["wout"] = (state_h, state), (wout_h, wout)
    plan["own"] = (resid_h.at[:, columns(t, cols)], own)
    plan["gain"], plan["group"] = (gain2_h, gain), (group_h, grouter)
    plan["router"] = (router_h, router)
    for i, w in enumerate((wg, wu)):
        plan[f"up{i}"] = (w, wgu.at[:, :, i * ff : (i + 1) * ff] if fused else wgu.at[i])
    for k in range(nz):
        at = columns(2 * z_at[k] + c, cols)
        plan[f"down{k}"] = (wd.at[:, :, at], wdown.at[k, :, :ff, :])
        at = columns(2 * z_at[k] + 1 - c, cols)
        plan[f"give{k}"] = (wd.at[:, :, at], down_give.at[k])
    def sent(*kinds):
        for ref, sem in kinds:
            pltpu.make_async_copy(ref, ref, sem).wait()

    loads = {}
    for name, (src, dst) in plan.items():
        kind = name.rstrip("0123")
        known = loads.get(kind)
        sem = known[1] if known else wsem.at[len(loads)]
        loads[kind] = (together.get(kind, dst), sem)
        pltpu.make_async_copy(src, dst, sem).start()
        if name == "norm":
            sent(loads["resid"])

    def loaded(*names):
        sent(*(loads[name] for name in names))

    loaded("norm")
    wide = resid[...].astype(F32)
    factor = lax.rsqrt(jnp.mean(wide * wide, axis=-1, keepdims=True) + EPSILON)
    normed = (wide * factor * gain1[...]).astype(BF16)
    for j in range(n):
        blocks[j] = normed[:, j * depth : (j + 1) * depth]
    half = rows // 2
    mine = pl.ds(pl.multiple_of(c * half, half), half)
    pl.semaphore_wait(pltpu.get_barrier_semaphore(), 1 + (n - 1) + (nz - 1))
    ahead, across = {}, {}
    for r in away:
        ahead[r] = remote(
            blocks.at[flip(me, r), mine, :], arrived.at[r, mine, :], as_, ar.at[r - 1], peers[r]
        )
        ahead[r].start()
    loaded("w", "gi", "gf", "bias", "running", "ids")
    acc[0] = dot(blocks[me], weights[...])
    for which, g in enumerate((gi, gf)):
        value = row_dot(g[...], normed)
        for j in range(nt):
            gates[which, j] = value[j * heads : (j + 1) * heads]
    for j in range(heads):
        line = slice(j, j + 1)
        in_gate = gates[0, t, line, :]
        forget = jax.nn.log_sigmoid(gates[1, t, line, :] + bias[t * heads + j])
        moved = forget + running[line, :]
        stable = jnp.maximum(moved, in_gate)
        new_max[line, :] = stable
        fades[0, line, :] = jnp.exp(moved - stable)
        fades[1, line, :] = jnp.exp(in_gate - stable)
    proj[...] = jnp.zeros(proj.shape, BF16)
    for r in away:
        ahead[r].wait_recv()
        across[r] = remote(
            arrived.at[r, mine, :], arrived.at[r, mine, :], qs_, qr.at[r - 1], partner
        )
        across[r].start()
    loaded("wout", "give")
    lend = []
    for k in range(nz):
        at = columns(2 * z_at[k] + 1 - c, cols)
        lend.append(remote(wout.at[:, at], wout_far.at[k], ls.at[0], lr.at[0], partner))
        lend.append(
            remote(down_give.at[k], wdown.at[k, :, ff:, :], ls.at[1], lr.at[1], partner)
        )
    for copy in lend:
        copy.start()
    expert_id = lax.broadcasted_iota(jnp.int32, (experts, rows), 0)
    picks = [ids[j : j + 1, :] == expert_id for j in range(ids.shape[0])]
    member = functools.reduce(jnp.logical_or, picks)
    member_f = member.astype(F32)
    before = (
        lax.broadcasted_iota(jnp.int32, (rows, rows), 0)
        < lax.broadcasted_iota(jnp.int32, (rows, rows), 1)
    ).astype(BF16)
    slot = dot(member_f.astype(BF16), before)
    slot = jnp.where(member, slot, -1.0)
    slot_id = lax.broadcasted_iota(jnp.int32, (cap, rows), 0).astype(F32)
    hots = []
    for e in range(experts):
        hots.append((slot[e : e + 1, :] == slot_id).astype(F32))
        chosen[e // local, e % local] = hots[e].astype(BF16)
    for j in range(n):
        block = jnp.concatenate(hots[j * local : (j + 1) * local], axis=0)
        scatter[j] = block.T.astype(BF16)


    parts = halving(n, 4 * width)
    wide_part = 4 * width // len(parts)
    back = {}

    def summed_part(b, p, r, position):
        value = acc[r, lots[b], p * wide_part : (p + 1) * wide_part]
        for s in range(position):
            bit = 1 << parts[p][s]
            back[b, p, r | bit].wait_recv()
            value = value + rcv[b, r | bit, p].astype(F32)
        return value

    steps = {}
    for r in range(1, n):
        for p in range(len(parts)):
            position = min(s for s, bit in enumerate(parts[p]) if r >> bit & 1)
            steps.setdefault((position, -weight_of(r)), []).append((r, p, position))
    order = []
    for i, key in enumerate(sorted(steps)):
        for b in range(batches):
            order.append((max(0, 2 * i - 1) if b == 0 else 2 * i + 2 * b, b, steps[key]))
    ready = {0}
    for _, b, step in sorted(order, key=lambda item: item[:2]):
        for r, p, position in step:
            if r not in ready:
                across[r].wait_recv()
                acc[r] = dot(arrived[r], weights[...])
                ready.add(r)
            snd[b, r, p] = summed_part(b, p, r, position).astype(BF16)
            back[b, p, r] = remote(
                snd.at[b, r, p], rcv.at[b, r, p], xs, xr.at[b, p, r - 1],
                peers[1 << parts[p][position]],
            )
            back[b, p, r].start()

    group = 8
    edge = min(128, heads * size)

    def read(b):
        for p in range(len(parts)):
            value = summed_part(b, p, 0, len(parts[p]))
            proj[lots[b], p * wide_part : (p + 1) * wide_part] = value.astype(BF16)
        for i, dst in enumerate((qs, ks, vs)):
            for j in range(0, width, edge):
                value = proj[:, i * width + j : i * width + j + edge].astype(F32).T
                dst[j : j + edge, :] = value * size ** (-0.5) if i == 0 else value
        for h in range(heads):
            lines = slice(h * size, (h + 1) * size)
            carried, fresh = fades[0, h : h + 1, :], fades[1, h : h + 1, :]
            q = qs[lines, :]
            score = jnp.sum(q * ks[lines, :], axis=0, keepdims=True) * fresh
            denom = carried * jnp.sum(q * normer[h], axis=0, keepdims=True) + score

            def some(g, readout, h=h):
                start = pl.multiple_of(g * group, group)
                q8 = qs[pl.ds(h * size + start, group), :]
                for i in range(group):
                    readout = readout + q8[i : i + 1, :] * state[h, start + i]
                return readout

            readout = lax.fori_loop(0, size // group, some, jnp.zeros(q.shape, F32))
            value = carried * readout + score * vs[lines, :]
            value = value / jnp.maximum(jnp.abs(denom), 1.0)
            mean = jnp.mean(value * value, axis=0, keepdims=True)
            cell[lines, :] = value * lax.rsqrt(mean + EPSILON)
        for j in range(0, width, edge):
            gate = jax.nn.sigmoid(proj[lots[b], 3 * width + j : 3 * width + j + edge].astype(F32))
            value = cell[j : j + edge, :].T[lots[b], :] * hgain[:, j : j + edge] * gate
            head[lots[b], j : j + edge] = value.astype(BF16)

    def renew():
        for h in range(heads):
            lines = slice(h * size, (h + 1) * size)
            carried, fresh = fades[0, h : h + 1, :], fades[1, h : h + 1, :]
            key = fresh * ks[lines, :]
            ks[lines, :] = key
            new_normer[h] = carried * normer[h] + key

            def some(g, x, h=h, carried=carried):
                start = pl.multiple_of(g * group, group)
                k8 = ks[pl.ds(h * size + start, group), :]
                v = vs[h * size : (h + 1) * size, :]
                for i in range(group):
                    new_matrix[h, start + i] = (
                        carried * state[h, start + i] + k8[i : i + 1, :] * v
                    )
                return x

            lax.fori_loop(0, size // group, some, 0)

    pair, reduce, total = {}, {}, {}

    def mix(b):
        pair[b] = remote(
            head.at[lots[b], :], head_far.at[lots[b], :], ps, pr.at[b], partner
        )
        pair[b].start()
        values = {}
        for k in far + [0]:
            at = columns(2 * z_at[k] + c, cols)
            values[k] = dot(head[lots[b], :], wout[:, at])
        pair[b].wait_recv()
        for k in far + [0]:
            value = values[k] + dot(head_far[lots[b], :], wout_far[k])
            if k > 0:
                for h in range(sides):
                    red_s[b, k, h] = value[:, bands[h]].astype(BF16)
            else:
                total[b] = value + own[lots[b], :].astype(F32)
        for h in range(sides):
            for k in far:
                reduce[b, k, h] = remote(
                    red_s.at[b, k, h], red_r.at[b, k, h], rs, rr.at[b, h], z_peers[k]
                )
                reduce[b, k, h].start()

    loaded("hgain", "normer", "state", "own")
    sent((wout_far, lr.at[0]))
    for b in range(batches):
        read(b)
        mix(b)
    share = {}
    for r in away:
        share[r] = remote(chosen.at[flip(me, r)], chosen_r.at[r], hs, hr, peers[r])
        share[r].start()
    renew()
    loaded("gain", "group", "router")
    gather = {}

    def collect(h):
        for b in range(batches):
            value = total[b][:, bands[h]]
            sent((red_r.at[b, 1:, h], rr.at[b, h]))
            for k in near:
                value = value + red_r[b, k, h].astype(F32)
            gathered[h, 0, lots[b], :] = value.astype(BF16)
        for k in near[:1] + far[:-1]:
            gather[h, k] = remote(
                gathered.at[h, 0], gathered.at[h, k], gs, gr.at[h, k - 1], z_peers[k]
            )
            gather[h, k].start()

    send, pass_on = {}, {}
    ones = jnp.ones((8, band), BF16)

    def lanes_of(h, k, side):
        start = (2 * z_at[k] + side) * cols + h * band
        return pl.ds(pl.multiple_of(start, band), band)

    def dispatch(h, k):
        if k > 0:
            gather[h, k].wait_recv()
        at = lanes_of(h, k, c)
        raw = gathered[h, k].astype(F32)
        scaled = (raw * gain[:, at]).astype(BF16)
        taken = dot(chosen[...].reshape(experts * cap, rows), scaled).astype(BF16)
        disp[h, k] = taken.reshape(n, local, cap, band)
        for r in away:
            send[h, k, r] = remote(
                disp.at[h, k, flip(me, r)], arr.at[c, h, k, :, r], ds, dr.at[h, k], peers[r]
            )
            send[h, k, r].start()
        arr[c, h, k, :, 0] = disp[h, k, me]
        square = raw * raw
        high = square.astype(BF16)
        low = (square - high.astype(F32)).astype(BF16)
        parts = (
            row_dot(ones, high) + row_dot(ones, low),
            row_dot(grouter[:, at], scaled),
            row_dot(router[:, at], scaled),
        )
        for base, part in zip((0, 8, 16), parts):
            lines = slice(base, base + part.shape[0])
            if k + h == 0:
                stat[lines, :] = part
            else:
                stat[lines, :] += part

    def forward(h, k):
        ref = arr.at[c, h, k, :, 1:]
        sent((ref, dr.at[h, k]))
        ref = arr.at[c, h, k]
        pass_on[h, k] = remote(ref, ref, fs, fr.at[h, k], partner)
        pass_on[h, k].start()
        widen(h, k, c)

    def settle_pass(h, k):
        pass_on[h, k].wait_recv()
        widen(h, k, 1 - c)

    def widen(h, k, side):
        at = lanes_of(h, k, side)
        for e in range(local):
            x = arr[side, h, k, e].reshape(n * cap, band)
            if fused:
                parts = [(slice(0, 2 * ff), dot(x, wgu[e, at, :]))]
            else:
                parts = [
                    (slice(i * ff, (i + 1) * ff), dot(x, wgu[i, e, at, :])) for i in range(2)
                ]
            for lanes, part in parts:
                if first[0]:
                    hidden[e, :, lanes] = part
                else:
                    hidden[e, :, lanes] += part
        first[0] = False

    note, swaps = {}, []

    def announce():
        swap = remote(stat, stat_r, ss, sr, partner)
        swap.start()
        swaps.append(swap)
        swap.wait_recv()

        def summed(base, count):
            lines = slice(base, base + count)
            return stat[lines, :] + stat_r[lines, :]

        factor = lax.rsqrt(summed(0, 1) * (1.0 / (cols * nt)) + EPSILON)
        group_exp = jnp.exp(summed(8, groups) * factor)
        group_prob = group_exp / jnp.sum(group_exp, axis=0, keepdims=True)
        logits = summed(16, experts) * factor
        group_id = lax.broadcasted_iota(jnp.int32, (groups, rows), 0)
        chosen_exp = [
            jnp.exp(jnp.sum(jnp.where(pick, logits, 0.0), axis=0, keepdims=True)) for pick in picks
        ]
        denominator = functools.reduce(jnp.add, chosen_exp)
        expert_weight = jnp.zeros((experts, rows), F32)
        for j, pick in enumerate(picks):
            group_hot = lax.div(ids[j : j + 1, :], per_group) == group_id
            group_share = jnp.sum(jnp.where(group_hot, group_prob, 0.0), axis=0, keepdims=True)
            expert_weight += jnp.where(pick, group_share * (chosen_exp[j] / denominator), 0.0)
        for j in range(n):
            msg[j, 0:1, :] = factor
            msg[j, 1 : 1 + local, :] = expert_weight[j * local : (j + 1) * local, :]
        for r in away:
            note[r] = remote(msg.at[flip(me, r)], msg_r.at[r], ms, mr, peers[r])
            note[r].start()

    first = [True]
    items = [(h, 0) for h in range(sides)]
    items += [(h, k) for k in near[:1] for h in range(sides)]
    items += [(h, k) for h in range(sides) for k in far[:-1]]
    for i, (h, k) in enumerate(items):
        if k == 0:
            collect(h)
        dispatch(h, k)
    announce()
    loaded("up")
    for i in range(len(items)):
        forward(*items[i])
        if i > 0:
            settle_pass(*items[i - 1])
    columns_of = [[] for _ in range(local)]
    weights_of = [[] for _ in range(local)]
    for r in range(n):
        if r == 1:
            sent((chosen_r.at[1:], hr), (msg_r.at[1:], mr))
        for e in range(local):
            hot = (chosen[me, e] if r == 0 else chosen_r[r, e]).astype(F32)
            words = msg[me] if r == 0 else msg_r[r]
            columns_of[e].append(jnp.sum(hot * words[0:1, :], axis=1, keepdims=True))
            weights_of[e].append(jnp.sum(hot * words[1 + e : 2 + e, :], axis=1, keepdims=True))
    settle_pass(*items[-1])
    share_units = []
    for e in range(local):
        scale = jnp.concatenate(columns_of[e], axis=0)
        weight = jnp.concatenate(weights_of[e], axis=0)
        gate = hidden[e, :, :ff] * scale
        up = hidden[e, :, ff:] * scale
        units[0, e] = (jax.nn.silu(gate) * up * weight).astype(BF16)
        copy = remote(units.at[0, e], units.at[1, e], es, er.at[e], partner)
        copy.start()
        share_units.append(copy)

    loaded("down")
    sent((down_give, lr.at[1]))
    for copy in share_units:
        copy.wait_recv()
    ret, gather_z = {}, {}
    if ff % 128 == 0:
        both = [jnp.concatenate([units[0, e], units[1, e]], axis=1) for e in range(local)]
    for k in far + [0]:
        for e in range(local):
            if ff % 128 == 0:
                value = dot(both[e], wdown[k, e])
            else:
                value = dot(units[0, e], wdown[k, e, :ff, :]) + dot(
                    units[1, e], wdown[k, e, ff:, :]
                )
            value = value.astype(BF16).reshape(n, cap, cols)
            for h in range(sides):
                ret_s[k, h, e] = value[:, :, bands[h]]
        for h in range(sides):
            for r in away:
                ret[k, h, r] = remote(
                    ret_s.at[k, h, :, r], ret_r.at[k, h, :, r], bs, br.at[k, h], peers[r]
                )
                ret[k, h, r].start()
    sent((arrived.at[1:, :half, :], as_), (arrived.at[1:, :half, :], qs_))
    sent((snd.at[:, 1:], xs), (head, ps), (red_s.at[:, 1:], rs), (gathered.at[:, 1:], gs))
    sent((chosen_r.at[1:], hs), (msg_r.at[1:], ms), (disp.at[:, :, 1:], ds), (arr.at[c], fs))
    sent((stat, ss), (units.at[0], es), (wout_far, ls.at[0]), (down_give, ls.at[1]))
    for k in far + [0]:
        for h in range(sides):
            total = gathered[h, 0].astype(F32) if k == 0 else None
            sent((ret_r.at[k, h, :, 1:], br.at[k, h]))
            for r in range(n):
                answer = ret_s[k, h, :, 0] if r == 0 else ret_r[k, h, :, r]
                part = dot(scatter[flip(me, r)], answer.reshape(local * cap, band))
                total = part if total is None else total + part
            if k > 0:
                z_s[k, h] = total.astype(BF16)
                gather_z[k, h] = remote(
                    z_s.at[k, h], z_r.at[k, h], zs, zr.at[h], z_peers[k]
                )
                gather_z[k, h].start()
            else:
                sent((z_r.at[1:, h], zr.at[h]))
                for k_from in far:
                    total = total + z_r[k_from, h].astype(F32)
                out[:, bands[h]] = total.astype(BF16)
    sent((ret_s.at[:, :, :, 1:], bs), (z_s.at[1:], zs))


def layer(
    resid, gain1, wq, wk, wv, wo, gi, gf, bias, hgain, running, normer, state, wout,
    gain2, group_router, expert_router, ids, wg, wu, wd,
):
    n, nt = lax.axis_size("ep"), lax.axis_size("tp")
    nz = nt // 2
    rows, channels = resid.shape
    cols = channels // nt
    depth, width = wq.shape
    heads = state.shape[0]
    local, _, ff = wg.shape
    experts = n * local
    groups = group_router.shape[0]
    topk = ids.shape[0]
    cap = max(2, 3 * rows * topk // (2 * experts))
    cap = -(-cap // 16) * 16
    lines = 16 + -(-experts // 8) * 8
    words = -(-(1 + local) // 8) * 8
    wide = (local, channels, 2 * ff) if ff % 128 == 0 else (2, local, channels, ff)
    parts = len(halving(n, 4 * width))
    batches = 2 if rows % 32 == 0 else 1
    lot = rows // batches
    vmem = pltpu.VMEM
    sides = 2 if cols % 256 == 0 else 1
    band = cols // sides
    reduced = (batches, nz, sides, lot, band)
    returned = (batches, n, parts, lot, 4 * width // parts)
    by_head = (width, rows)
    arrays = (
        resid, gain1, wq, wk, wv, wo, gi, gf, bias, hgain, running, normer, state, wout,
        gain2, group_router, expert_router, ids, wg, wu, wd,
    )
    return pl.pallas_call(
        functools.partial(layer_kernel, n, nt, cap, groups, experts // groups),
        out_shape=(
            vmem((rows, cols), BF16),
            vmem(state.shape, F32),
            vmem(normer.shape, F32),
            vmem(running.shape, F32),
        ),
        in_specs=[HBM] * len(arrays),
        out_specs=(VMEM,) * 4,
        scratch_shapes=[
            vmem((rows, channels), BF16),
            vmem((1, channels), F32),
            vmem(gi.shape, BF16),
            vmem(gf.shape, BF16),
            pltpu.SMEM(bias.shape, F32),
            vmem(hgain.shape, F32),
            vmem(running.shape, F32),
            vmem(normer.shape, F32),
            vmem(state.shape, F32),
            vmem(wout.shape, BF16),
            vmem((1, channels), F32),
            vmem(group_router.shape, BF16),
            vmem(expert_router.shape, BF16),
            vmem(ids.shape, jnp.int32),
            vmem((depth, 4 * width), BF16),
            vmem(wide, BF16),
            vmem((nz, local, 2 * ff, cols), BF16),
            vmem((n, rows, depth), BF16),
            vmem((n, rows, depth), BF16),
            vmem((n, rows, 4 * width), F32),
            vmem(returned, BF16),
            vmem(returned, BF16),
            vmem((2, nt, heads, rows), F32),
            vmem((rows, 4 * width), BF16),
            vmem(by_head, F32),
            vmem(by_head, F32),
            vmem(by_head, F32),
            vmem(by_head, F32),
            vmem((2, heads, rows), F32),
            vmem((rows, width), BF16),
            vmem((rows, cols), BF16),
            vmem((n, local, cap, rows), BF16),
            vmem((n, local, cap, rows), BF16),
            vmem((n, rows, local * cap), BF16),
            vmem((nz, width, cols), BF16),
            vmem((nz, local, ff, cols), BF16),
            vmem((rows, width), BF16),
            vmem((2, local, n * cap, ff), BF16),
            vmem(reduced, BF16),
            vmem(reduced, BF16),
            vmem((sides, nz, rows, band), BF16),
            vmem((sides, nz, n, local, cap, band), BF16),
            vmem((2, sides, nz, local, n, cap, band), BF16),
            vmem((lines, rows), F32),
            vmem((lines, rows), F32),
            vmem((n, words, rows), F32),
            vmem((n, words, rows), F32),
            vmem((local, n * cap, 2 * ff), F32),
            vmem((nz, sides, local, n, cap, band), BF16),
            vmem((nz, sides, local, n, cap, band), BF16),
            vmem((nz, sides, rows, band), BF16),
            vmem((nz, sides, rows, band), BF16),
            DMA((len(arrays),)),
            DMA, DMA((n - 1,)), DMA, DMA((n - 1,)), DMA, DMA((batches, parts, n - 1)),
            DMA, DMA, DMA, DMA((batches,)), DMA((2,)), DMA((2,)),
            DMA, DMA((batches, sides)),
            DMA, DMA((sides, nz - 1)), DMA, DMA((sides, nz)), DMA, DMA((sides, nz)),
            DMA, DMA, DMA, DMA,
            DMA, DMA((local,)), DMA, DMA((nz, sides)), DMA, DMA((sides,)),
        ],
        compiler_params=pltpu.CompilerParams(
            collective_id=0, has_side_effects=True, vmem_limit_bytes=52 * 1024 * 1024,
        ),
    )(*in_hbm(*arrays))


def settle_kernel(mixed, matrix, normer, highest, *refs):
    sems = refs[-1]
    pairs = list(zip((mixed, normer, highest), (refs[0], refs[2], refs[3])))
    heads, size = matrix.shape[:2]
    step = size // 4
    for h in range(heads):
        for i in range(0, size, step):
            pairs.append((matrix.at[h, i : i + step], refs[1].at[h, i : i + step]))
    copies = [pltpu.make_async_copy(*pair, sems.at[i]) for i, pair in enumerate(pairs)]
    for copy in copies:
        copy.start()
    for copy in copies:
        copy.wait()


def settle(*arrays):
    return pl.pallas_call(
        settle_kernel,
        out_shape=tuple(pltpu.HBM(a.shape, a.dtype) for a in arrays),
        in_specs=[VMEM] * len(arrays),
        out_specs=(HBM,) * len(arrays),
        scratch_shapes=[DMA((3 + 4 * arrays[1].shape[0],))],
        compiler_params=pltpu.CompilerParams(vmem_limit_bytes=12 * 1024 * 1024),
    )(*in_vmem(*arrays))


def per_device(
    resid,
    norm1_gain,
    w_query,
    w_key,
    w_value,
    w_outgate,
    w_igate,
    w_fgate,
    forget_bias,
    head_gain,
    w_out,
    state_matrix,
    state_norm,
    state_max,
    norm2_gain,
    group_router,
    expert_router,
    expert_ids,
    exp_gate,
    exp_up,
    exp_down,
):
    mixed, new_matrix, new_normer, new_max = settle(
        *layer(
            resid, norm1_gain.reshape(1, -1), w_query, w_key, w_value, w_outgate,
            w_igate.T, w_fgate.T, forget_bias, head_gain.reshape(1, -1), state_max.T,
            state_norm.transpose(1, 2, 0), state_matrix.transpose(1, 2, 3, 0), w_out,
            norm2_gain.reshape(1, -1), group_router.T, expert_router.T, expert_ids.T,
            exp_gate, exp_up, exp_down,
        )
    )
    return (
        mixed, new_matrix.transpose(3, 0, 1, 2), new_normer.transpose(2, 0, 1), new_max.T
    )


def solution(mesh):
    in_specs = (
        P("ep", None),
        P(),
        P("ep", "tp"),
        P("ep", "tp"),
        P("ep", "tp"),
        P("ep", "tp"),
        P(),
        P(),
        P(),
        P("tp"),
        P("tp", None),
        P("ep", "tp", None, None),
        P("ep", "tp", None),
        P("ep", "tp"),
        P(),
        P(),
        P(),
        P("ep", None),
        P("ep", None, "tp"),
        P("ep", None, "tp"),
        P("ep", "tp", None),
    )
    out_specs = (P("ep", "tp"), P("ep", "tp", None, None), P("ep", "tp", None), P("ep", "tp"))
    return jax.shard_map(
        per_device, mesh=mesh, in_specs=in_specs, out_specs=out_specs, check_vma=False
    )
```
